512 devices in a mesh: sp: 64 (over z, y), tp: 8 (over x, core).
Axes of the slice: x: 4, y: 8, z: 8, core: 2. Of those that a mesh axis runs over, the one named last changes fastest.
Arguments:
- activations: bfloat16 [16384, 2048], P('sp', 'tp'), may hold values from -170 to 170
- norm_gain: float32 [2048], replicated, may hold values from 0.1 to 1.9
- query_weight: bfloat16 [2048, 1536], P(None, 'tp'), may hold values from -0.125 to 0.125
- latent_weight: bfloat16 [2048, 512], P(None, 'tp'), may hold values from -0.125 to 0.125
- rope_key_weight: bfloat16 [2048, 64], replicated, may hold values from -0.125 to 0.125
- latent_gain: float32 [512], replicated, may hold values from 1.5 to 64
- expand_weight: bfloat16 [512, 2048], P(None, 'tp'), may hold values from -0.25 to 0.25
- gate_weight: bfloat16 [2048, 1024], P(None, 'tp'), may hold values from -0.125 to 0.125
- pre_weight: bfloat16 [2048, 1024], P(None, 'tp'), may hold values from -0.125 to 0.125
- value_weight: bfloat16 [2048, 1024], P(None, 'tp'), may hold values from -0.125 to 0.125
- conv_kernel: bfloat16 [3, 1024], P(None, 'tp'), may hold values from -3.5 to 3.5
- output_attend: bfloat16 [1024, 2048], P('tp'), may hold values from -0.1875 to 0.1875
- output_conv: bfloat16 [1024, 2048], P('tp'), may hold values from -0.125 to 0.125
Outputs:
- mixed: bfloat16 [16384, 2048], P(('sp', 'tp'))
- log_weight_sum: float32 [8, 16384], P('tp', 'sp')
The draws below stay inside these ranges and needn't reach their ends.
All inputs are finite; a program needn't handle non-finite values.
Results may differ from the reference program's by a relative error of at most 0.035.
The reference program's roundings to bfloat16 on the way count: a program that leaves them out, or rounds other values in their place, can miss the bound.
Values may be sent and summed in bfloat16 or wider, within the bound.
A program may use at most 128 MiB of HBM per device.

```python
import math
import jax
import jax.numpy as jnp
from jax import lax

D = 2048
HEADS = 8
NOPE = 128
ROPE = 64
VDIM = 128
KV_RANK = 512
CONV_CH = 1024
KERNEL = 3
GRID_W = 64
TOKENS = 16384
N_TP = 8


def draw_activations(key, part):
    noise_key = jax.random.fold_in(key, 11)
    scale_key = jax.random.fold_in(key, 12)
    steps_along = jnp.arange(D, dtype=jnp.float32) / D
    noise = jnp.clip(jax.random.normal(noise_key, (TOKENS, D), jnp.float32), -5.0, 5.0)
    column_scale = 3.0 ** steps_along
    row_scale = jnp.exp(jax.random.uniform(scale_key, (TOKENS, 1), jnp.float32, 0.0, 1.1))
    return (noise * column_scale * row_scale).astype(jnp.bfloat16)


def draw_latent_gain(key, part):
    gain_key = jax.random.fold_in(key, 21)
    lower_end = math.log(1.5)
    upper_end = math.log(6.0)
    return jnp.exp(jax.random.uniform(gain_key, (KV_RANK,), jnp.float32, lower_end, upper_end))


def level_of(rng, extent, cuts, least, largest):
    loudness, own = 1.0, jax.random.fold_in(rng, 6)
    for position, parts in cuts:
        heights = jnp.exp(jax.random.uniform(jax.random.fold_in(own, position), (parts,), jnp.float32, least / len(cuts), largest / len(cuts)))
        loudness = loudness * jnp.repeat(heights, extent[position] // parts).reshape([-1 if axis == position else 1 for axis in range(len(extent))])
    return loudness


def scatter_about(stream_key, shape, deviation, limit, shards=(), kind=jnp.bfloat16):
    entries = deviation * jax.random.normal(stream_key, shape, jnp.float32)
    if shards:
        entries = entries * level_of(stream_key, shape, shards, -0.22, 0.18)
    return jnp.clip(entries, -limit, limit).astype(kind)


def setup_inputs(seed: int = 0) -> dict:
    key_of = jax.random.split(jax.random.key(seed), 14)
    activations = draw_activations(jax.random.fold_in(key_of[13], 71), 0)
    norm_gain = jnp.clip(1.0 + 0.18 * jax.random.normal(key_of[1], (D,), jnp.float32), 0.1, 1.9)
    query_weight = scatter_about(key_of[2], (D, HEADS * (NOPE + ROPE)), D ** -0.5, 0.125, ((1, 8),))
    latent_weight = scatter_about(key_of[3], (D, KV_RANK), D ** -0.5, 0.125, ((1, 8),))
    rope_key_weight = scatter_about(key_of[4], (D, ROPE), D ** -0.5, 0.125)
    latent_gain = draw_latent_gain(jax.random.fold_in(key_of[13], 71), 0)
    expand_weight = scatter_about(key_of[6], (KV_RANK, HEADS * (NOPE + VDIM)), KV_RANK ** -0.5, 0.25, ((1, 8),))
    gate_weight = scatter_about(key_of[7], (D, CONV_CH), D ** -0.5, 0.125, ((1, 8),))
    pre_weight = scatter_about(key_of[8], (D, CONV_CH), D ** -0.5, 0.125, ((1, 8),))
    value_weight = scatter_about(key_of[9], (D, CONV_CH), D ** -0.5, 0.125, ((1, 8),))
    conv_kernel = scatter_about(key_of[10], (KERNEL, CONV_CH), KERNEL ** -0.5, 3.5, ((1, 8),))
    output_attend = scatter_about(key_of[11], (HEADS * VDIM, D), (HEADS * VDIM) ** -0.5, 0.1875, ((0, 8),))
    output_conv = scatter_about(key_of[12], (CONV_CH, D), (2 * CONV_CH) ** -0.5, 0.125, ((0, 8),))
    return {"activations": activations, "norm_gain": norm_gain, "query_weight": query_weight, "latent_weight": latent_weight, "rope_key_weight": rope_key_weight, "latent_gain": latent_gain, "expand_weight": expand_weight, "gate_weight": gate_weight, "pre_weight": pre_weight, "value_weight": value_weight, "conv_kernel": conv_kernel, "output_attend": output_attend, "output_conv": output_conv}


EPSILON = 1e-06
ROPE_BASE = 10000.0

def rotate(inputs, grid_rows, grid_cols):
    quarter = inputs.shape[-1] // 4
    inverse = ROPE_BASE ** (-jnp.arange(quarter, dtype=jnp.float32) / quarter)
    row_angle = (grid_rows[:, None] * inverse)[:, None, :]
    col_angle = (grid_cols[:, None] * inverse)[:, None, :]
    part_one = inputs[..., :quarter]
    part_two = inputs[..., quarter:2 * quarter]
    part_three = inputs[..., 2 * quarter:3 * quarter]
    part_four = inputs[..., 3 * quarter:]
    return jnp.concatenate([part_one * jnp.cos(row_angle) - part_two * jnp.sin(row_angle), part_one * jnp.sin(row_angle) + part_two * jnp.cos(row_angle), part_three * jnp.cos(col_angle) - part_four * jnp.sin(col_angle), part_three * jnp.sin(col_angle) + part_four * jnp.cos(col_angle)], axis=-1)

def reference(activations, norm_gain, query_weight, latent_weight, rope_key_weight, latent_gain, expand_weight, gate_weight, pre_weight, value_weight, conv_kernel, output_attend, output_conv):
    inputs_f32 = activations.astype(jnp.float32)
    scaled = (inputs_f32 * norm_gain).astype(jnp.bfloat16)
    inv_rms = lax.rsqrt(lax.optimization_barrier(jnp.mean(inputs_f32 * inputs_f32, axis=1, keepdims=True)) + EPSILON)

    def project(weight):
        return jnp.dot(scaled, weight, preferred_element_type=jnp.float32) * inv_rms
    positions = jnp.arange(TOKENS, dtype=jnp.int32)
    grid_rows = (positions // GRID_W).astype(jnp.float32)
    grid_cols = (positions % GRID_W).astype(jnp.float32)
    query = project(query_weight).reshape(TOKENS, HEADS, NOPE + ROPE)
    query = jnp.concatenate([query[..., :NOPE], rotate(query[..., NOPE:], grid_rows, grid_cols)], axis=-1)
    query = (query * (NOPE + ROPE) ** (-0.5)).astype(jnp.bfloat16)
    latent_part = project(latent_weight).astype(jnp.bfloat16).astype(jnp.float32)
    latent = (latent_part * lax.rsqrt(lax.optimization_barrier(jnp.mean(latent_part * latent_part, axis=1, keepdims=True)) + EPSILON) * latent_gain).astype(jnp.bfloat16)
    expanded = jnp.dot(latent, expand_weight, preferred_element_type=jnp.float32).astype(jnp.bfloat16)
    expanded = expanded.reshape(TOKENS, HEADS, NOPE + VDIM)
    rope_key = rotate(project(rope_key_weight)[:, None, :], grid_rows, grid_cols)[:, 0].astype(jnp.bfloat16)
    key_nope = expanded[..., :NOPE].astype(jnp.float32)
    values = expanded[..., NOPE:].astype(jnp.float32)
    rope_f32 = rope_key.astype(jnp.float32)
    query_block = math.gcd(TOKENS, 512)
    query_blocks = query.reshape(TOKENS // query_block, query_block, HEADS, NOPE + ROPE)

    def attend(block):
        block_f32 = block.astype(jnp.float32)
        scores = jnp.einsum('thd,jhd->htj', block_f32[..., :NOPE], key_nope)
        scores = scores + jnp.einsum('thd,jd->htj', block_f32[..., NOPE:], rope_f32)
        row_max = lax.optimization_barrier(jnp.max(scores, axis=-1))
        shifted = jnp.exp(scores - row_max[..., None])
        row_sum = lax.optimization_barrier(jnp.sum(shifted, axis=-1))
        weights = lax.optimization_barrier(shifted.astype(jnp.bfloat16)).astype(jnp.float32)
        summed = jnp.einsum('htj,jhd->thd', weights, values)
        attended_block = (summed / row_sum.T[..., None]).astype(jnp.bfloat16)
        return (attended_block, row_max + jnp.log(row_sum))
    attended_blocks, log_blocks = lax.map(attend, query_blocks)
    attended = attended_blocks.reshape(TOKENS, HEADS * VDIM)
    log_weight_sum = jnp.transpose(log_blocks, (1, 0, 2)).reshape(HEADS, TOKENS)
    pre_mix = (project(pre_weight) * project(value_weight)).astype(jnp.bfloat16).astype(jnp.float32)
    padded = jnp.pad(pre_mix, ((1, 1), (0, 0)))
    kernel = conv_kernel.astype(jnp.float32)
    convolved = kernel[0] * padded[:-2] + kernel[1] * padded[1:-1] + kernel[2] * padded[2:]
    conv_mixed = (project(gate_weight) * convolved).astype(jnp.bfloat16)
    attend_cols = HEADS * VDIM // N_TP
    conv_cols = CONV_CH // N_TP
    summed_out = jnp.zeros((TOKENS, D), jnp.float32)
    for group_index in range(N_TP):
        head_part = attended[:, group_index * attend_cols:(group_index + 1) * attend_cols]
        chan_part = conv_mixed[:, group_index * conv_cols:(group_index + 1) * conv_cols]
        partial_value = jnp.dot(head_part, output_attend[group_index * attend_cols:(group_index + 1) * attend_cols], preferred_element_type=jnp.float32)
        partial_value = partial_value + jnp.dot(chan_part, output_conv[group_index * conv_cols:(group_index + 1) * conv_cols], preferred_element_type=jnp.float32)
        summed_out = summed_out + lax.optimization_barrier(partial_value.astype(jnp.bfloat16)).astype(jnp.float32)
    mixed = summed_out.astype(jnp.bfloat16)
    return (mixed, log_weight_sum)
```

```python
import functools

import jax
import jax.numpy as jnp
import numpy as np
from jax import lax
from jax.experimental import pallas as pl
from jax.experimental.pallas import tpu as pltpu
from jax.sharding import PartitionSpec as P

MESH = pl.DeviceIdType.MESH
F32 = jnp.float32
BF16 = jnp.bfloat16

D = 2048
NOPE = 128
ROPE = 64
GRID_W = 64
EPSILON = 1e-06
ROPE_BASE = 10000.0
RING = 8
NX = 4
T = 256
Q_ROWS, Q_CHUNKS = 384, 2
KV_ROWS, KV_CHUNKS = 640, 4
LOW = -3.0e38


def rotation_tables():
    inverse = (np.float32(ROPE_BASE) ** (-np.arange(16, dtype=np.float32) / np.float32(16))).astype(np.float32)
    quarter = np.arange(128) // 16 % 4
    freq = inverse[np.arange(128) % 16]
    sign = np.where(quarter % 2 == 0, -1.0, 1.0)

    def table(count, mask):
        angle = (np.arange(count, dtype=np.float32)[:, None] * freq[None, :]).astype(np.float32)
        angle = angle.astype(np.float64)
        return np.concatenate([np.cos(angle) * mask, np.sin(angle) * sign * mask], axis=1).astype(np.float32)

    return table(256, quarter < 2), table(GRID_W, quarter >= 2)


def lane_iota(rows):
    return lax.broadcasted_iota(jnp.int32, (rows, 128), 1)


def kernel(
    act_hbm, gain_hbm, qw_hbm, lw_hbm, rw_hbm, lgain_hbm, ew_hbm, gw_hbm, pw_hbm, vw_hbm, ck_hbm, oa_hbm, oc_hbm,
    rowtab_hbm, coltab_hbm,
    mixed_ref, lws_ref,
    act_all, gain, qw, lw, rw, lgain, ew, wcat, ck, wout, rowtab, coltab, acc, lat_all,
    q_all, qr_all, kv_all, kr_all, vt_all, stats, o_acc, o_send, o_recv, st_recv,
    halo_out, halo_in, cat, e_psend, e_precv, e_own, e_xsend, e_xrecv,
    load_sem, a_send, a_recv, l_send, l_recv, q_send, q_recv, kv_send, kv_recv, d_send, d_recv,
    h_send, h_recv, ep_send, ep_recv, ex_send, ex_recv,
):
    sp = lax.axis_index("sp")
    tp = lax.axis_index("tp")
    x, c = lax.div(tp, 2), lax.rem(tp, 2)
    z, y = lax.div(sp, RING), lax.rem(sp, RING)
    ka, qa = y + c * (z - y), z + c * (y - z)
    k_stride, q_stride = 1 + 7 * c, 8 - 7 * c

    def ring(pos, offset):
        return lax.rem(pos + (offset + RING), RING)

    def k_dev(offset):
        return (sp + (ring(ka, offset) - ka) * k_stride, tp)

    def q_dev(offset):
        return (sp + (ring(qa, offset) - qa) * q_stride, tp)

    def chip(offset):
        return lax.rem(x + offset, NX)

    def t_dev(xx, cc):
        return (sp, 2 * xx + cc)

    sends = []

    def remote(src, dst, send, recv, dev):
        return pltpu.make_async_remote_copy(
            src_ref=src, dst_ref=dst, send_sem=send, recv_sem=recv, device_id=dev, device_id_type=MESH
        )

    def push(src, dst, send, recv, dev):
        copy = remote(src, dst, send, recv, dev)
        copy.start()
        sends.append(copy)

    def arrived(dst, send, recv, dev):
        remote(dst, dst, send, recv, dev).wait_recv()

    loads = []
    for i, (src, dst) in enumerate(
        [
            (act_hbm, act_all.at[tp]),
            (qw_hbm, qw),
            (rw_hbm, rw),
            (lw_hbm, lw),
            (gw_hbm, wcat.at[:, pl.ds(256, 128)]),
            (pw_hbm, wcat.at[:, pl.ds(384, 128)]),
            (vw_hbm, wcat.at[:, pl.ds(512, 128)]),
            (gain_hbm, gain),
            (lgain_hbm, lgain),
            (rowtab_hbm, rowtab),
            (coltab_hbm, coltab),
            (ck_hbm, ck),
            (ew_hbm, ew),
            (oa_hbm, wout.at[pl.ds(0, 128), :]),
            (oc_hbm, wout.at[pl.ds(128, 128), :]),
        ]
    ):
        copy = pltpu.make_async_copy(src, dst, load_sem.at[i])
        copy.start()
        loads.append(copy)

    barrier = pltpu.get_barrier_semaphore()
    partners = [(sp, lax.rem(tp + k, 8)) for k in range(1, 8)]
    partners += [q_dev(k) for k in range(1, 8)] + [k_dev(1), k_dev(-1)]
    after, before = (lax.rem(sp + 1, 64), tp), (lax.rem(sp + 63, 64), tp)
    partners += [after, before]
    for dev in partners:
        pl.semaphore_signal(barrier, inc=1, device_id=dev, device_id_type=MESH)
    loads[0].wait()
    pl.semaphore_wait(barrier, len(partners))

    def half(slot, h):
        return act_all.at[slot, pl.ds(128 * h, 128), :]

    count = [0]

    def a_push(slot, h, dev):
        push(half(slot, h), half(slot, h), a_send.at[count[0]], a_recv.at[slot, h], dev)
        count[0] += 1

    def a_wait(slot, h):
        arrived(half(slot, h), a_send.at[0], a_recv.at[slot, h], t_dev(x, 1 - c))

    up, down, mate = t_dev(chip(1), c), t_dev(chip(3), c), t_dev(x, 1 - c)
    a_push(tp, 0, up)
    a_push(tp, 1, down)
    a_push(tp, 0, mate)
    a_push(tp, 1, mate)
    a_push(tp, 1, up)
    a_push(tp, 0, down)

    for copy in loads[1:8]:
        copy.wait()

    def assemble(i, _):
        rows = pl.ds(i * 256, 256)
        wcat[rows, 0:128] = qw[rows, 0:128]
        wcat[rows, 128:256] = jnp.concatenate([qw[rows, 128:192], rw[rows, :]], axis=1)
        wcat[rows, 640:768] = jnp.concatenate([lw[rows, :], lw[rows, :]], axis=1)
        return 0

    lax.fori_loop(0, D // 256, assemble, 0)

    def project(slot, first):
        piece = act_all[slot].astype(F32)
        scaled = (piece * gain[:, pl.ds(pl.multiple_of(slot * 256, 256), 256)]).astype(BF16)
        part = jnp.dot(scaled, wcat[pl.ds(pl.multiple_of(slot * 256, 256), 256), :], preferred_element_type=F32)
        acc[...] = part if first else acc[...] + part
        squares = piece * piece
        return squares[:, 0:128] + squares[:, 128:256]

    squares = project(tp, True)
    s_down, s_up, s_far = 2 * chip(3) + c, 2 * chip(1) + c, 2 * chip(2) + c
    other = 1 - 2 * c
    a_wait(s_down, 0)
    a_push(s_down, 0, up)
    a_push(s_down, 0, mate)
    a_wait(s_up, 1)
    a_push(s_up, 1, down)
    a_push(s_up, 1, mate)
    for h in range(2):
        a_wait(tp + other, h)
    squares += project(tp + other, False)
    a_wait(s_down, 1)
    a_push(s_down, 1, mate)
    a_wait(s_up, 0)
    a_push(s_up, 0, mate)
    squares += project(s_down, False)
    squares += project(s_up, False)
    for slot in (s_down, s_up):
        for h in range(2):
            a_wait(slot + other, h)
        squares += project(slot + other, False)
    for h in range(2):
        a_wait(s_far, h)
        a_push(s_far, h, mate)
    squares += project(s_far, False)
    for h in range(2):
        a_wait(s_far + other, h)
    squares += project(s_far + other, False)
    inv_rms = lax.rsqrt(jnp.sum(squares, axis=1, keepdims=True) / D + EPSILON)

    low = lane_iota(128) < 64
    latent_part = acc[:, 640:768] * inv_rms
    lat_all[tp] = jnp.where(low, latent_part[0:128], latent_part[128:256]).astype(BF16)

    def l_push(i, slot, dev):
        push(lat_all.at[slot], lat_all.at[slot], l_send.at[i], l_recv.at[slot], dev)

    def l_wait(slot):
        arrived(lat_all.at[slot], l_send.at[0], l_recv.at[slot], mate)

    for i, dev in enumerate((t_dev(chip(2), c), up, down, mate)):
        l_push(i, tp, dev)

    for copy in loads[8:]:
        copy.wait()
    scale = (NOPE + ROPE) ** (-0.5)
    q_all[qa, 0:256, :] = (acc[:, 0:128] * inv_rms * scale).astype(BF16)
    raw = acc[:, 128:256] * inv_rms
    even = lax.rem(lax.div(lane_iota(T), 16), 2) == 0
    tables = [rowtab[pl.ds(sp * 4 + g, 1), :] + coltab[...] for g in range(4)]
    tables = jnp.concatenate(tables, axis=0)
    turned = jnp.where(even, pltpu.roll(raw, 112, 1), pltpu.roll(raw, 16, 1))
    rotated = raw * tables[:, 0:128] + turned * tables[:, 128:256]
    swapped = pltpu.roll(rotated, 64, 1)
    q_all[qa, 256:384, :] = (jnp.where(low, rotated[0:128], swapped[128:256]) * scale).astype(BF16)

    def chunks_of(direction, step, chunks):
        if step < 4:
            return range(chunks)
        return range(chunks // 2) if direction == 1 else range(chunks // 2, chunks)

    def ring_push(blocks, pos, rows, chunks, send, recv, dev, step):
        n = rows // chunks
        for ch in range(chunks):
            for d in (1, -1):
                if ch in chunks_of(d, step + 1, chunks):
                    part = blocks.at[ring(pos, -d * step), pl.ds(ch * n, n), :]
                    push(part, part, send.at[(1 - d) // 2, step, ch], recv.at[ring(pos, -d * step), ch], dev(d))

    def ring_step(blocks, pos, rows, chunks, send, recv, dev, step, ch):
        n = rows // chunks
        for d in (1, -1):
            if ch in chunks_of(d, step, chunks):
                slot = ring(pos, -d * step)
                part = blocks.at[slot, pl.ds(ch * n, n), :]
                arrived(part, send.at[0, 0, 0], recv.at[slot, ch], dev(d))
                if step < 4 and ch in chunks_of(d, step + 1, chunks):
                    push(part, part, send.at[(1 - d) // 2, step, ch], recv.at[slot, ch], dev(d))

    q_ring = (q_all, qa, Q_ROWS, Q_CHUNKS, q_send, q_recv, q_dev)
    kv_ring = (kv_all, ka, KV_ROWS, KV_CHUNKS, kv_send, kv_recv, k_dev)
    ring_push(*q_ring, 0)

    def open_query(slot):
        paired = q_all[slot, 256:384, :].astype(F32)
        qr_all[slot, 0:128, :] = jnp.where(low, paired, 0.0).astype(BF16)
        qr_all[slot, 128:256, :] = jnp.where(low, pltpu.roll(paired, 64, 1), 0.0).astype(BF16)

    def open_keys(slot):
        paired = kv_all[slot, 256:384, :]
        kr_all[slot, 0:128, :] = paired
        kr_all[slot, 128:256, :] = pltpu.roll(paired.astype(F32), 64, 1).astype(BF16)
        vt_all[slot] = jnp.transpose(kv_all[slot, 384:640, :].astype(F32)).astype(BF16)

    pre_mix = (acc[:, 384:512] * inv_rms) * (acc[:, 512:640] * inv_rms)
    pre_mix = pre_mix.astype(BF16).astype(F32)
    halo_out[0] = pre_mix[0:8]
    halo_out[1] = pre_mix[248:256]
    push(halo_out.at[0], halo_in.at[1], h_send.at[0], h_recv.at[1], before)
    push(halo_out.at[1], halo_in.at[0], h_send.at[1], h_recv.at[0], after)
    gate = acc[:, 256:384] * inv_rms

    kv_rope = jnp.where(low, swapped[0:128], rotated[128:256]).astype(BF16)
    kv_all[ka, 256:384, :] = kv_rope
    open_query(qa)
    stats[:, 0:1, :] = jnp.full((8, 1, T), LOW, F32)
    stats[:, 1:8, :] = jnp.zeros((8, 7, T), F32)
    o_acc[...] = jnp.zeros_like(o_acc)
    for i, slot in enumerate((s_down, s_up, s_far)):
        l_wait(slot)
        l_push(4 + i, slot, mate)
    for slot in (tp, s_down, s_up, s_far):
        l_wait_slot = slot + other
        l_wait(l_wait_slot)

    def pair(j):
        a, b = lat_all[2 * j].astype(F32), lat_all[2 * j + 1].astype(F32)
        return jnp.concatenate(
            [jnp.where(low, a, pltpu.roll(b, 64, 1)), jnp.where(low, pltpu.roll(a, 64, 1), b)], axis=0
        )

    parts = jnp.concatenate([pair(j) for j in range(4)], axis=1)
    latent_inv = lax.rsqrt(jnp.mean(parts * parts, axis=1, keepdims=True) + EPSILON)
    latent = (parts * latent_inv * lgain[...]).astype(BF16)
    expanded = jnp.dot(latent, ew[...], preferred_element_type=F32).astype(BF16)
    kv_all[ka, 0:256, :] = expanded[:, 0:128]
    kv_all[ka, 384:640, :] = expanded[:, 128:256]
    ring_push(*kv_ring, 0)

    for i in range(2):
        arrived(halo_in.at[i], h_send.at[0], h_recv.at[i], after)
    row = lax.broadcasted_iota(jnp.int32, (T, 128), 0)
    first = jnp.where(sp > 0, halo_in[0, 7:8, :], 0.0)
    last = jnp.where(sp < 63, halo_in[1, 0:1, :], 0.0)
    shifted_down = jnp.where(row == 0, first, pltpu.roll(pre_mix, 1, 0))
    shifted_up = jnp.where(row == T - 1, last, pltpu.roll(pre_mix, T - 1, 0))
    taps = ck[...].astype(F32)
    convolved = taps[0:1] * shifted_down + taps[1:2] * pre_mix + taps[2:3] * shifted_up
    cat[:, 128:256] = (gate * convolved).astype(BF16)
    open_keys(ka)

    def unit(qs, k, last_block):
        keys = jnp.concatenate([kv_all[k, 0:256, :], kr_all[k]], axis=1)
        values = vt_all[k]
        results = []
        for q in qs:
            queries = jnp.concatenate([q_all[q, 0:256, :], qr_all[q]], axis=1)
            scores = lax.dot_general(keys, queries, (((1,), (1,)), ((), ())), preferred_element_type=F32)
            old_max, old_sum = stats[q, 0:1, :], stats[q, 1:2, :]
            new_max = jnp.maximum(old_max, jnp.max(scores, axis=0, keepdims=True))
            rescale = jnp.exp(old_max - new_max)
            weights = jnp.exp(scores - new_max)
            new_sum = old_sum * rescale + jnp.sum(weights, axis=0, keepdims=True)
            out = jnp.dot(values, weights.astype(BF16), preferred_element_type=F32)
            results.append((new_max, new_sum, o_acc[q] * rescale + out))
        for q, (new_max, new_sum, out) in zip(qs, results):
            stats[q, 0:1, :] = new_max
            stats[q, 1:2, :] = new_sum
            o_acc[q] = out
            if last_block:
                o_send[q] = out.astype(BF16)

    def q_pair(p):
        return ring(qa, p), lax.rem(qa + RING - lax.rem(p, 4), RING)

    def units(pairs, keys):
        p0, pn = pairs
        k0, dk, kn = keys

        def step(i, _):
            p = p0 + lax.rem(i, pn)
            unit(q_pair(p), ring(ka, k0 + dk * lax.div(i, pn) + RING), False)
            return 0

        lax.fori_loop(0, pn * kn, step, 0)

    def q_step(step):
        for ch in range(Q_CHUNKS):
            ring_step(*q_ring, step, ch)
        for slot in {1: (ring(qa, step), ring(qa, -step))}.get(int(step < 4), (ring(qa, 4),)):
            open_query(slot)

    def kv_step(step):
        for ch in range(KV_CHUNKS):
            ring_step(*kv_ring, step, ch)
        for slot in {1: (ring(ka, step), ring(ka, -step))}.get(int(step < 4), (ring(ka, 4),)):
            open_keys(slot)

    q_step(1)
    units((1, 1), (0, 1, 1))
    q_step(2)
    kv_step(1)
    units((2, 1), (0, 1, 1))
    units((1, 2), (-1, 2, 2))
    q_step(3)
    units((3, 1), (-1, 1, 3))
    kv_step(2)
    units((1, 3), (-2, 4, 2))
    q_step(4)
    units((4, 1), (-2, 1, 5))
    kv_step(3)
    units((1, 4), (-3, 6, 2))
    kv_step(4)

    def d_push(offset):
        slot = ring(qa, offset)
        push(o_send.at[slot], o_recv.at[qa], d_send.at[offset, 0], d_recv.at[qa, 0], q_dev(offset))
        push(stats.at[slot], st_recv.at[qa], d_send.at[offset, 1], d_recv.at[qa, 1], q_dev(offset))

    for p in (4, 3, 2, 1):
        unit(q_pair(p), ring(ka, 4), True)
        d_push(p)
        if p < 4:
            d_push(8 - p)
    for offset in range(1, 8):
        slot = ring(qa, offset)
        arrived(o_recv.at[slot], d_send.at[1, 0], d_recv.at[slot, 0], q_dev(offset))
        arrived(st_recv.at[slot], d_send.at[1, 1], d_recv.at[slot, 1], q_dev(offset))
    whole_max = stats[qa, 0:1, :]
    for offset in range(1, 8):
        whole_max = jnp.maximum(whole_max, st_recv[ring(qa, offset), 0:1, :])
    weight = jnp.exp(stats[qa, 0:1, :] - whole_max)
    whole_sum = stats[qa, 1:2, :] * weight
    whole_out = o_acc[qa] * weight
    for offset in range(1, 8):
        slot = ring(qa, offset)
        weight = jnp.exp(st_recv[slot, 0:1, :] - whole_max)
        whole_sum += st_recv[slot, 1:2, :] * weight
        whole_out += o_recv[slot].astype(F32) * weight
    lws_ref[...] = whole_max + jnp.log(whole_sum)
    cat[:, 0:128] = jnp.transpose(whole_out / whole_sum).astype(BF16)

    def rows_of(xx, cc):
        return pl.ds(pl.multiple_of((2 * xx + cc) * 32, 32), 32)

    order = [chip(2), chip(1), chip(3), x]
    for_mate = jnp.concatenate([cat[rows_of(xx, 1 - c), :] for xx in order], axis=0)
    for n in range(4):
        cols = slice(512 * n, 512 * n + 512)
        part = jnp.dot(for_mate, wout[:, cols], preferred_element_type=F32).astype(BF16)
        for j in range(4):
            e_psend[j, :, cols] = part[32 * j : 32 * j + 32]
    for j in range(4):
        push(e_psend.at[j], e_precv.at[j], ep_send.at[j], ep_recv.at[j], mate)
    for_own = jnp.concatenate([cat[rows_of(xx, c), :] for xx in order], axis=0)
    for n in range(4):
        cols = slice(512 * n, 512 * n + 512)
        part = jnp.dot(for_own, wout[:, cols], preferred_element_type=F32)
        for j in range(4):
            e_own[j, :, cols] = part[32 * j : 32 * j + 32]
    for j in range(3):
        arrived(e_precv.at[j], ep_send.at[0], ep_recv.at[j], mate)
        e_xsend[j] = (e_own[j] + e_precv[j].astype(F32)).astype(BF16)
        push(e_xsend.at[j], e_xrecv.at[j], ex_send.at[j], ex_recv.at[j], t_dev(order[j], c))
    arrived(e_precv.at[3], ep_send.at[0], ep_recv.at[3], mate)
    total = e_own[3] + e_precv[3].astype(F32)
    for j in (1, 2, 0):
        arrived(e_xrecv.at[j], ex_send.at[0], ex_recv.at[j], t_dev(order[j], c))
        total += e_xrecv[j].astype(F32)
    mixed_ref[...] = total.astype(BF16)
    for copy in sends:
        copy.wait_send()


def body(
    activations, norm_gain, query_weight, latent_weight, rope_key_weight, latent_gain, expand_weight,
    gate_weight, pre_weight, value_weight, conv_kernel, output_attend, output_conv,
):
    rowtab, coltab = rotation_tables()
    dma = pltpu.SemaphoreType.DMA
    vmem = pltpu.VMEM
    return pl.pallas_call(
        kernel,
        out_shape=(jax.ShapeDtypeStruct((32, D), BF16), jax.ShapeDtypeStruct((1, T), F32)),
        in_specs=[pl.BlockSpec(memory_space=pl.ANY)] * 15,
        out_specs=(pl.BlockSpec(memory_space=vmem), pl.BlockSpec(memory_space=vmem)),
        scratch_shapes=[
            vmem((8, T, 256), BF16),
            vmem((1, D), F32),
            vmem((D, 192), BF16),
            vmem((D, 64), BF16),
            vmem((D, 64), BF16),
            vmem((1, 512), F32),
            vmem((512, 256), BF16),
            vmem((D, 768), BF16),
            vmem((3, 128), BF16),
            vmem((256, D), BF16),
            vmem((256, 256), F32),
            vmem((64, 256), F32),
            vmem((T, 768), F32),
            vmem((8, 128, 128), BF16),
            vmem((8, Q_ROWS, 128), BF16),
            vmem((8, T, 128), BF16),
            vmem((8, KV_ROWS, 128), BF16),
            vmem((8, T, 128), BF16),
            vmem((8, 128, T), BF16),
            vmem((8, 8, T), F32),
            vmem((8, 128, T), F32),
            vmem((8, 128, T), BF16),
            vmem((8, 128, T), BF16),
            vmem((8, 8, T), F32),
            vmem((2, 8, 128), F32),
            vmem((2, 8, 128), F32),
            vmem((T, 256), BF16),
            vmem((4, 32, D), BF16),
            vmem((4, 32, D), BF16),
            vmem((4, 32, D), F32),
            vmem((3, 32, D), BF16),
            vmem((3, 32, D), BF16),
            dma((15,)),
            dma((14,)),
            dma((8, 2)),
            dma((7,)),
            dma((8,)),
            dma((2, 4, Q_CHUNKS)),
            dma((8, Q_CHUNKS)),
            dma((2, 4, KV_CHUNKS)),
            dma((8, KV_CHUNKS)),
            dma((8, 2)),
            dma((8, 2)),
            dma((2,)),
            dma((2,)),
            dma((4,)),
            dma((4,)),
            dma((3,)),
            dma((3,)),
        ],
        compiler_params=pltpu.CompilerParams(collective_id=0, has_side_effects=True),
    )(
        activations, norm_gain.reshape(1, D), query_weight, latent_weight, rope_key_weight,
        latent_gain.reshape(1, 512), expand_weight, gate_weight, pre_weight, value_weight, conv_kernel,
        output_attend, output_conv, jnp.asarray(rowtab), jnp.asarray(coltab),
    )


def solution(mesh):
    return jax.shard_map(
        body,
        mesh=mesh,
        in_specs=(
            P("sp", "tp"),
            P(),
            P(None, "tp"),
            P(None, "tp"),
            P(),
            P(),
            P(None, "tp"),
            P(None, "tp"),
            P(None, "tp"),
            P(None, "tp"),
            P(None, "tp"),
            P("tp", None),
            P("tp", None),
        ),
        out_specs=(P(("sp", "tp"), None), P("tp", "sp")),
        check_vma=False,
    )
```

```python
import functools

import jax
import jax.numpy as jnp
import numpy as np
from jax import lax
from jax.experimental import pallas as pl
from jax.experimental.pallas import tpu as pltpu
from jax.sharding import PartitionSpec as P

MESH = pl.DeviceIdType.MESH
F32 = jnp.float32
BF16 = jnp.bfloat16

D = 2048
NOPE = 128
ROPE = 64
GRID_W = 64
EPSILON = 1e-06
ROPE_BASE = 10000.0
RING = 8
NX = 4
T = 256
Q_ROWS = 384
KV_ROWS, KV_CHUNKS = 640, 4
V_ROWS = 144
LOW = -3.0e38
LOG2E = 1.4426950408889634


def rotation_tables():
    inverse = (np.float32(ROPE_BASE) ** (-np.arange(16, dtype=np.float32) / np.float32(16))).astype(np.float32)
    quarter = np.arange(128) // 16 % 4
    freq = inverse[np.arange(128) % 16]
    sign = np.where(quarter % 2 == 0, -1.0, 1.0)

    def table(count, mask):
        angle = (np.arange(count, dtype=np.float32)[:, None] * freq[None, :]).astype(np.float32)
        angle = angle.astype(np.float64)
        return np.concatenate([np.cos(angle) * mask, np.sin(angle) * sign * mask], axis=1).astype(np.float32)

    return np.concatenate([table(256, quarter < 2), table(GRID_W, quarter >= 2)])


def lane_iota(rows):
    return lax.broadcasted_iota(jnp.int32, (rows, 128), 1)


def kernel(
    act_hbm, gain_hbm, qw_hbm, lw_hbm, rw_hbm, lgain_hbm, ew_hbm, gw_hbm, pw_hbm, vw_hbm, ck_hbm, oa_hbm, oc_hbm,
    table_hbm,
    mixed_ref, lws_ref,
    act_all, gain, lgain, ew, wt, wb, ck, wout, table, acc, acc_b, lat_all,
    q_all, q_cat, kv_all, k_cat, vt_all, s_buf, w_buf, r_buf, stats, o_acc, o_send, o_recv, st_recv,
    halo_out, halo_in, cat, e_psend, e_precv, e_own, e_xsend, e_xrecv,
    load_sem, sent, a_recv, l_recv, q_recv, kv_recv, d_recv, h_recv, ep_recv, ex_recv,
):
    sp = lax.axis_index("sp")
    tp = lax.axis_index("tp")
    x, c = lax.div(tp, 2), lax.rem(tp, 2)
    z, y = lax.div(sp, RING), lax.rem(sp, RING)
    ka, qa = y + c * (z - y), z + c * (y - z)
    k_stride, q_stride = 1 + 7 * c, 8 - 7 * c

    def ring(pos, offset):
        return lax.rem(pos + (offset + RING), RING)

    def k_dev(offset):
        return (sp + (ring(ka, offset) - ka) * k_stride, tp)

    def q_dev(offset):
        return (sp + (ring(qa, offset) - qa) * q_stride, tp)

    def chip(offset):
        return lax.rem(x + offset, NX)

    def t_dev(xx, cc):
        return (sp, 2 * xx + cc)

    scopes = []
    A, L, Q, KV, O, ST, EP, EX, H = (sent.at[i] for i in range(9))

    def phase(name):
        if scopes:
            scopes.pop().__exit__(None, None, None)
        if name:
            scopes.append(jax.named_scope(name))
            scopes[-1].__enter__()

    def remote(src, dst, send, recv, dev):
        return pltpu.make_async_remote_copy(
            src_ref=src, dst_ref=dst, send_sem=send, recv_sem=recv, device_id=dev, device_id_type=MESH
        )

    def push(src, dst, send, recv, dev):
        remote(src, dst, send, recv, dev).start()

    def arrived(bytes_of, recv):
        remote(bytes_of, bytes_of, A, recv, t_dev(x, 1 - c)).wait_recv()

    phase("loads")
    def load(i, *pairs):
        for src, dst in pairs:
            pltpu.make_async_copy(src, dst, load_sem.at[i]).start()

    def loaded(i, ref):
        pltpu.make_async_copy(ref, ref, load_sem.at[i]).wait()

    load(0, (act_hbm, act_all.at[tp]))
    load(1, (gain_hbm, gain))
    load(
        2,
        (qw_hbm, wt.at[pl.ds(0, 192), :]),
        (rw_hbm, wt.at[pl.ds(192, 64), :]),
        (lw_hbm, wt.at[pl.ds(256, 64), :]),
        (lw_hbm, wt.at[pl.ds(320, 64), :]),
    )
    load(
        3,
        (gw_hbm, wb.at[:, pl.ds(0, 128)]),
        (pw_hbm, wb.at[:, pl.ds(128, 128)]),
        (vw_hbm, wb.at[:, pl.ds(256, 128)]),
    )
    load(4, (lgain_hbm, lgain))
    load(5, (table_hbm, table))
    load(6, (ck_hbm, ck))
    load(7, (ew_hbm, ew))
    load(8, (oa_hbm, wout.at[pl.ds(0, 128), :]), (oc_hbm, wout.at[pl.ds(128, 128), :]))

    phase("barrier")
    barrier = pltpu.get_barrier_semaphore()
    partners = [(sp, lax.rem(tp + k, 8)) for k in range(1, 8)]
    partners += [q_dev(k) for k in range(1, 8)] + [k_dev(1), k_dev(-1)]
    after, before = (lax.rem(sp + 1, 64), tp), (lax.rem(sp + 63, 64), tp)
    partners += [after, before]
    for dev in partners:
        pl.semaphore_signal(barrier, inc=1, device_id=dev, device_id_type=MESH)
    loaded(0, act_all.at[tp])
    pl.semaphore_wait(barrier, len(partners))

    phase("act_own")
    def rows_at(slot, ch, n):
        return act_all.at[slot, pl.ds(64 * ch, 64 * n), :]

    def a_push(slot, ch, n, recv, dev):
        push(rows_at(slot, ch, n), rows_at(slot, ch, n), A, a_recv.at[recv], dev)

    def a_wait(n, recv):
        arrived(act_all.at[0, pl.ds(0, 64 * n), :], a_recv.at[recv])

    up, down, mate = t_dev(chip(1), c), t_dev(chip(3), c), t_dev(x, 1 - c)
    for i in range(2):
        a_push(tp, i, 1, i, up)
        a_push(tp, 2 + i, 1, 3 + i, down)
    a_push(tp, 0, 4, 7, mate)
    a_push(tp, 2, 2, 2, up)
    a_push(tp, 0, 2, 5, down)
    loaded(1, gain)
    loaded(2, wt)
    loaded(3, wb)

    def project(slot, first):
        piece = act_all[slot].astype(F32)
        features = pl.ds(pl.multiple_of(slot * 256, 256), 256)
        scaled = (piece * gain[:, features]).astype(BF16)
        part = lax.dot_general(scaled, wt[:, features], (((1,), (1,)), ((), ())), preferred_element_type=F32)
        acc[...] = part if first else acc[...] + part
        part = jnp.dot(scaled, wb[features, :], preferred_element_type=F32)
        acc_b[...] = part if first else acc_b[...] + part
        squares = piece * piece
        return squares[:, 0:128] + squares[:, 128:256]

    squares = project(tp, True)
    phase("act_one")
    s_down, s_up, s_far = 2 * chip(3) + c, 2 * chip(1) + c, 2 * chip(2) + c
    other = 1 - 2 * c
    for i in range(2):
        a_wait(1, i)
        a_push(s_down, i, 1, 6, up)
        a_wait(1, 3 + i)
        a_push(s_up, 2 + i, 1, 6, down)
    a_wait(2, 2)
    a_push(s_down, 0, 4, 8, mate)
    a_wait(2, 5)
    a_push(s_up, 0, 4, 9, mate)
    a_wait(4, 7)
    squares += project(tp + other, False)
    squares += project(s_down, False)
    squares += project(s_up, False)
    a_wait(4, 8)
    squares += project(s_down + other, False)
    a_wait(4, 9)
    squares += project(s_up + other, False)
    phase("act_far")
    a_wait(4, 6)
    a_push(s_far, 0, 4, 10, mate)
    squares += project(s_far, False)
    a_wait(4, 10)
    squares += project(s_far + other, False)
    phase("latent_send")
    inv_rms = lax.rsqrt(jnp.sum(squares, axis=1, keepdims=True) / D + EPSILON)

    low = lane_iota(128) < 64
    latent_part = acc[:, 256:384] * inv_rms
    lat_all[tp] = jnp.where(low, latent_part[0:128], latent_part[128:256]).astype(BF16)

    def l_push(slot, recv, dev):
        push(lat_all.at[slot], lat_all.at[slot], L, l_recv.at[recv], dev)

    for i, dev in enumerate((t_dev(chip(2), c), up, down, mate)):
        l_push(tp, i, dev)

    phase("query")
    loaded(4, lgain)
    loaded(5, table)
    loaded(6, ck)
    loaded(7, ew)
    loaded(8, wout)
    scale = (NOPE + ROPE) ** (-0.5) * LOG2E
    q_all[qa, 0:256, :] = (acc[:, 0:128] * inv_rms * scale).astype(BF16)
    raw = acc[:, 128:256] * inv_rms
    even = lax.rem(lax.div(lane_iota(T), 16), 2) == 0
    tables = [table[pl.ds(sp * 4 + g, 1), :] + table[256:320, :] for g in range(4)]
    tables = jnp.concatenate(tables, axis=0)
    turned = jnp.where(even, pltpu.roll(raw, 112, 1), pltpu.roll(raw, 16, 1))
    rotated = raw * tables[:, 0:128] + turned * tables[:, 128:256]
    swapped = pltpu.roll(rotated, 64, 1)
    q_all[qa, 256:384, :] = (jnp.where(low, rotated[0:128], swapped[128:256]) * scale).astype(BF16)

    def q_push(offset, ch, n, recv, to):
        part = q_all.at[ring(qa, offset), pl.ds(192 * ch, 192 * n), :]
        push(part, part, Q, q_recv.at[recv], q_dev(to))

    def q_wait(n, recv):
        arrived(q_all.at[pl.ds(0, n)] if n else q_all.at[0, pl.ds(0, 192), :], q_recv.at[recv])

    q_push(0, 0, 2, 0, 1)
    q_push(0, 0, 2, 1, -1)
    q_push(0, 0, 1, 2, 2)
    q_push(0, 1, 1, 3, -2)
    q_push(0, 1, 1, 4, 2)
    q_push(0, 0, 1, 4, -2)

    n_kv = KV_ROWS // KV_CHUNKS

    def kv_push(step, ch, to):
        part = kv_all.at[ring(ka, -to * step), pl.ds(ch * n_kv, n_kv), :]
        recv = step * KV_CHUNKS + ch if step < 3 else 3 * KV_CHUNKS
        push(part, part, KV, kv_recv.at[recv], k_dev(to))

    def kv_step(step, some):
        for ch in some:
            arrived(kv_all.at[0, pl.ds(0, 2 * n_kv), :], kv_recv.at[(step - 1) * KV_CHUNKS + ch])
            if step < 3 or ch < KV_CHUNKS // 2:
                kv_push(step, ch, 1)
            if step < 3 or ch >= KV_CHUNKS // 2:
                kv_push(step, ch, -1)

    def open_query(slot):
        paired = q_all[slot, 256:384, :].astype(F32)
        q_cat[slot, :, 0:128] = q_all[slot, 0:256, :]
        q_cat[slot, 0:128, 128:256] = jnp.where(low, paired, 0.0).astype(BF16)
        q_cat[slot, 128:256, 128:256] = jnp.where(low, pltpu.roll(paired, 64, 1), 0.0).astype(BF16)

    def open_keys(slot):
        paired = kv_all[slot, 256:384, :]
        k_cat[slot, :, 0:128] = kv_all[slot, 0:256, :]
        k_cat[slot, 0:128, 128:256] = paired
        k_cat[slot, 128:256, 128:256] = pltpu.roll(paired.astype(F32), 64, 1).astype(BF16)
        vt_all[slot, 0:128, :] = jnp.transpose(kv_all[slot, 384:640, :].astype(F32)).astype(BF16)

    phase("halo")
    pre_mix = (acc_b[:, 128:256] * inv_rms) * (acc_b[:, 256:384] * inv_rms)
    pre_mix = pre_mix.astype(BF16).astype(F32)
    halo_out[0] = pre_mix[0:8]
    halo_out[1] = pre_mix[248:256]
    push(halo_out.at[0], halo_in.at[1], H, h_recv.at[0], before)
    push(halo_out.at[1], halo_in.at[0], H, h_recv.at[0], after)
    gate = acc_b[:, 0:128] * inv_rms

    phase("latent_wait")
    kv_rope = jnp.where(low, swapped[0:128], rotated[128:256]).astype(BF16)
    kv_all[ka, 256:384, :] = kv_rope
    open_query(qa)
    stats[:, 0:1, :] = jnp.full((8, 1, T), LOW, F32)
    stats[:, 1:8, :] = jnp.zeros((8, 7, T), F32)
    o_acc[...] = jnp.zeros_like(o_acc)
    ones = lax.broadcasted_iota(jnp.int32, (8, V_ROWS - 128, T), 1) == 0
    vt_all[:, 128:V_ROWS, :] = jnp.where(ones, 1.0, 0.0).astype(BF16)
    phase("q1")
    q_wait(1, 0)
    q_push(-1, 0, 2, 5, 2)
    q_wait(1, 1)
    q_push(1, 0, 2, 5, -2)
    phase("latent_x")
    for recv, slot in ((1, s_down), (2, s_up), (0, s_far)):
        arrived(lat_all.at[0], l_recv.at[recv])
        l_push(slot, 3, mate)
    phase("q2")
    q_wait(0, 2)
    q_push(-2, 0, 1, 6, 2)
    q_wait(0, 3)
    q_push(2, 1, 1, 6, -2)
    phase("latent_mate")
    arrived(lat_all.at[pl.ds(0, 4)], l_recv.at[3])

    def pair(j):
        a, b = lat_all[2 * j].astype(F32), lat_all[2 * j + 1].astype(F32)
        return jnp.concatenate(
            [jnp.where(low, a, pltpu.roll(b, 64, 1)), jnp.where(low, pltpu.roll(a, 64, 1), b)], axis=0
        )

    phase("expand")
    parts = jnp.concatenate([pair(j) for j in range(4)], axis=1)
    latent_inv = lax.rsqrt(jnp.mean(parts * parts, axis=1, keepdims=True) + EPSILON)
    latent = (parts * latent_inv * lgain[...]).astype(BF16)
    expanded = jnp.dot(latent, ew[...], preferred_element_type=F32).astype(BF16)
    kv_all[ka, 0:256, :] = expanded[:, 0:128]
    kv_all[ka, 384:640, :] = expanded[:, 128:256]
    for ch in range(KV_CHUNKS):
        kv_push(0, ch, 1)
        kv_push(0, ch, -1)

    phase("conv")
    arrived(halo_in, h_recv.at[0])
    row = lax.broadcasted_iota(jnp.int32, (T, 128), 0)
    first = jnp.where(sp > 0, halo_in[0, 7:8, :], 0.0)
    last = jnp.where(sp < 63, halo_in[1, 0:1, :], 0.0)
    shifted_down = jnp.where(row == 0, first, pltpu.roll(pre_mix, 1, 0))
    shifted_up = jnp.where(row == T - 1, last, pltpu.roll(pre_mix, T - 1, 0))
    taps = ck[...].astype(F32)
    convolved = taps[0:1] * shifted_down + taps[1:2] * pre_mix + taps[2:3] * shifted_up
    cat[:, 128:256] = (gate * convolved).astype(BF16)
    open_keys(ka)

    phase("q_rest")
    first_chunks, other_chunks = range(KV_CHUNKS // 2), range(KV_CHUNKS // 2, KV_CHUNKS)
    q_wait(1, 4)
    for offset in (1, -1, 2, -2):
        open_query(ring(qa, offset))
    phase("q3")
    q_wait(2, 5)
    for offset in (3, -3):
        open_query(ring(qa, offset))
    phase("q4")
    q_wait(1, 6)
    open_query(ring(qa, 4))

    def key_blocks(ks, qs):
        n = len(ks) * T
        keys = jnp.concatenate([k_cat[k] for k in ks], axis=0)
        values = jnp.concatenate([vt_all[k] for k in ks], axis=1)
        for i, q in enumerate(qs):
            s_buf[i, 0:n] = lax.dot_general(keys, q_cat[q], (((1,), (1,)), ((), ())), preferred_element_type=F32)
        for i, q in enumerate(qs):
            scores = s_buf[i, 0:n]
            old_max = stats[q, 0:1, :]
            new_max = jnp.maximum(old_max, jnp.max(scores, axis=0, keepdims=True))
            r_buf[i, 0:1, :] = jnp.exp2(old_max - new_max)
            stats[q, 0:1, :] = new_max
            w_buf[i, 0:n] = jnp.exp2(scores - new_max).astype(BF16)
        for i, q in enumerate(qs):
            yield o_acc[q] * r_buf[i, 0:1, :] + jnp.dot(values, w_buf[i, 0:n], preferred_element_type=F32)

    def d_push(offset):
        slot = ring(qa, offset)
        push(o_send.at[slot], o_recv.at[qa], O, d_recv.at[0], q_dev(offset))
        push(stats.at[slot], st_recv.at[qa], ST, d_recv.at[1], q_dev(offset))

    def key_step(step, _):
        for s in (1, 2, 3):

            @pl.when(step == s)
            def _(s=s):
                kv_step(s, other_chunks if s == 1 else range(KV_CHUNKS))
                for d in (s, -s):
                    open_keys(ring(ka, d))

        ks = (lax.rem(ka + step, RING), lax.rem(ka - step + RING, RING))
        for q, out in enumerate(key_blocks(ks, range(8))):
            o_acc[q] = out
        return 0

    phase("k1")
    kv_step(1, first_chunks)
    phase("own_keys")
    for q, out in enumerate(key_blocks((ka,), range(8))):
        o_acc[q] = out
    phase("keys")
    lax.fori_loop(1, 4, key_step, 0)
    phase("k4")
    arrived(kv_all.at[0], kv_recv.at[3 * KV_CHUNKS])
    open_keys(ring(ka, 4))
    phase("last_keys")
    offsets = (4, 3, 5, 2, 6, 1, 7, 0)
    qs = [ring(qa, offset) for offset in offsets]
    for i, out in enumerate(key_blocks((ring(ka, 4),), qs)):
        stats[qs[i], 1:2, :] = out[128:129]
        if offsets[i]:
            o_send[qs[i]] = out[0:128].astype(BF16)
        else:
            o_acc[qa] = out
        if i in (2, 4, 6):
            for offset in offsets[0 if i == 2 else i - 1 : i + 1]:
                d_push(offset)
    phase("d_wait")
    arrived(st_recv.at[pl.ds(0, 7)], d_recv.at[1])
    arrived(o_recv.at[pl.ds(0, 7)], d_recv.at[0])
    phase("merge")
    whole_max = stats[qa, 0:1, :]
    for offset in range(1, 8):
        whole_max = jnp.maximum(whole_max, st_recv[ring(qa, offset), 0:1, :])
    weight = jnp.exp2(stats[qa, 0:1, :] - whole_max)
    whole_sum = stats[qa, 1:2, :] * weight
    whole_out = o_acc[qa, 0:128, :] * weight
    for offset in range(1, 8):
        slot = ring(qa, offset)
        weight = jnp.exp2(st_recv[slot, 0:1, :] - whole_max)
        whole_sum += st_recv[slot, 1:2, :] * weight
        whole_out += o_recv[slot].astype(F32) * weight
    lws_ref[...] = whole_max * (1.0 / LOG2E) + jnp.log(whole_sum)
    cat[:, 0:128] = jnp.transpose(whole_out / whole_sum).astype(BF16)

    phase("out_mate")
    def rows_of(xx, cc):
        return pl.ds(pl.multiple_of((2 * xx + cc) * 32, 32), 32)

    order = [chip(2), chip(1), chip(3), x]
    for_mate = jnp.concatenate([cat[rows_of(xx, 1 - c), :] for xx in order], axis=0)
    for n in range(4):
        cols = slice(512 * n, 512 * n + 512)
        part = jnp.dot(for_mate, wout[:, cols], preferred_element_type=F32).astype(BF16)
        for j in range(4):
            e_psend[j, :, cols] = part[32 * j : 32 * j + 32]
    for j in range(4):
        push(e_psend.at[j], e_precv.at[j], EP, ep_recv.at[j], mate)
    phase("out_own")
    for_own = jnp.concatenate([cat[rows_of(xx, c), :] for xx in order], axis=0)
    for n in range(4):
        cols = slice(512 * n, 512 * n + 512)
        part = jnp.dot(for_own, wout[:, cols], preferred_element_type=F32)
        for j in range(4):
            e_own[j, :, cols] = part[32 * j : 32 * j + 32]
    phase("e_mate")
    for j in range(3):
        arrived(e_precv.at[j], ep_recv.at[j])
        e_xsend[j] = (e_own[j] + e_precv[j].astype(F32)).astype(BF16)
        push(e_xsend.at[j], e_xrecv.at[j], EX, ex_recv.at[0], t_dev(order[j], c))
    phase("e_sum")
    arrived(e_precv.at[3], ep_recv.at[3])
    total = e_own[3] + e_precv[3].astype(F32)
    arrived(e_xrecv, ex_recv.at[0])
    for j in (1, 2, 0):
        total += e_xrecv[j].astype(F32)
    mixed_ref[...] = total.astype(BF16)
    phase("send_wait")
    for ref, send in (
        (act_all.at[pl.ds(0, 7)], A),
        (lat_all.at[pl.ds(0, 7)], L),
        (q_all.at[pl.ds(0, 7)], Q),
        (kv_all.at[pl.ds(0, 7)], KV),
        (o_send.at[pl.ds(0, 7)], O),
        (stats.at[pl.ds(0, 7)], ST),
        (e_psend, EP),
        (e_xsend, EX),
        (halo_out, H),
    ):
        remote(ref, ref, send, d_recv.at[0], mate).wait_send()
    phase(None)


def body(
    activations, norm_gain, query_weight, latent_weight, rope_key_weight, latent_gain, expand_weight,
    gate_weight, pre_weight, value_weight, conv_kernel, output_attend, output_conv,
):
    dma = pltpu.SemaphoreType.DMA
    vmem = pltpu.VMEM
    return pl.pallas_call(
        kernel,
        out_shape=(vmem((32, D), BF16), vmem((1, T), F32)),
        in_specs=[pl.BlockSpec(memory_space=pl.ANY)] * 14,
        out_specs=(pl.BlockSpec(memory_space=vmem), pl.BlockSpec(memory_space=vmem)),
        scratch_shapes=[
            vmem((8, T, 256), BF16),
            vmem((1, D), F32),
            vmem((1, 512), F32),
            vmem((512, 256), BF16),
            vmem((384, D), BF16),
            vmem((D, 384), BF16),
            vmem((3, 128), BF16),
            vmem((256, D), BF16),
            vmem((320, 256), F32),
            vmem((T, 384), F32),
            vmem((T, 384), F32),
            vmem((8, 128, 128), BF16),
            vmem((8, Q_ROWS, 128), BF16),
            vmem((8, T, 256), BF16),
            vmem((8, KV_ROWS, 128), BF16),
            vmem((8, T, 256), BF16),
            vmem((8, V_ROWS, T), BF16),
            vmem((8, 2 * T, T), F32),
            vmem((8, 2 * T, T), BF16),
            vmem((8, 8, T), F32),
            vmem((8, 8, T), F32),
            vmem((8, V_ROWS, T), F32),
            vmem((8, 128, T), BF16),
            vmem((8, 128, T), BF16),
            vmem((8, 8, T), F32),
            vmem((2, 8, 128), F32),
            vmem((2, 8, 128), F32),
            vmem((T, 256), BF16),
            vmem((4, 32, D), BF16),
            vmem((4, 32, D), BF16),
            vmem((4, 32, D), F32),
            vmem((3, 32, D), BF16),
            vmem((3, 32, D), BF16),
            dma((9,)),
            dma((9,)),
            dma((11,)),
            dma((4,)),
            dma((7,)),
            dma((3 * KV_CHUNKS + 1,)),
            dma((2,)),
            dma((1,)),
            dma((4,)),
            dma((1,)),
        ],
        compiler_params=pltpu.CompilerParams(collective_id=0, has_side_effects=True),
    )(
        activations, norm_gain.reshape(1, D), query_weight.T, latent_weight.T, rope_key_weight.T,
        latent_gain.reshape(1, 512), expand_weight, gate_weight, pre_weight, value_weight, conv_kernel,
        output_attend, output_conv, jnp.asarray(rotation_tables()),
    )


def solution(mesh):
    return jax.shard_map(
        body,
        mesh=mesh,
        in_specs=(
            P("sp", "tp"),
            P(),
            P(None, "tp"),
            P(None, "tp"),
            P(),
            P(),
            P(None, "tp"),
            P(None, "tp"),
            P(None, "tp"),
            P(None, "tp"),
            P(None, "tp"),
            P("tp", None),
            P("tp", None),
        ),
        out_specs=(P(("sp", "tp"), None), P("tp", "sp")),
        check_vma=False,
    )
```

```python
import functools

import jax
import jax.numpy as jnp
import numpy as np
from jax import lax
from jax.experimental import pallas as pl
from jax.experimental.pallas import tpu as pltpu
from jax.sharding import PartitionSpec as P

MESH = pl.DeviceIdType.MESH
F32 = jnp.float32
BF16 = jnp.bfloat16

D = 2048
NOPE = 128
ROPE = 64
GRID_W = 64
EPSILON = 1e-06
ROPE_BASE = 10000.0
RING = 8
NX = 4
T = 256
Q_ROWS = 384
KV_ROWS = 640
V_ROWS = 144
LOW = -3.0e38
LOG2E = 1.4426950408889634


def rotation_tables():
    inverse = (np.float32(ROPE_BASE) ** (-np.arange(16, dtype=np.float32) / np.float32(16))).astype(np.float32)
    quarter = np.arange(128) // 16 % 4
    freq = inverse[np.arange(128) % 16]
    sign = np.where(quarter % 2 == 0, -1.0, 1.0)

    def table(count, mask):
        angle = (np.arange(count, dtype=np.float32)[:, None] * freq[None, :]).astype(np.float32)
        angle = angle.astype(np.float64)
        return np.concatenate([np.cos(angle) * mask, np.sin(angle) * sign * mask], axis=1).astype(np.float32)

    return np.concatenate([table(256, quarter < 2), table(GRID_W, quarter >= 2)])


def lane_iota(rows):
    return lax.broadcasted_iota(jnp.int32, (rows, 128), 1)


def kernel(
    act_hbm, gain_hbm, qw_hbm, lw_hbm, rw_hbm, lgain_hbm, ew_hbm, gw_hbm, pw_hbm, vw_hbm, ck_hbm, oa_hbm, oc_hbm,
    table_hbm,
    mixed_ref, lws_ref,
    act_all, gain, lgain, ew, wt, wb, ck, wa_all, wc, table, acc, acc_b, lat_all,
    q_all, q_cat, kv_all, k_cat, vt_all, s_buf, w_buf, r_buf, stats, o_acc, o_send, o_recv, st_recv,
    halo_out, halo_in, conv_mixed, attended, heads, e_psend, e_precv, e_own, e_xsend, e_xrecv,
    load_sem, sent, a_recv, l_recv, q_recv, kv_recv, d_recv, h_recv, ep_recv, ex_recv, w_recv, at_recv,
):
    sp = lax.axis_index("sp")
    tp = lax.axis_index("tp")
    x, c = lax.div(tp, 2), lax.rem(tp, 2)
    z, y = lax.div(sp, RING), lax.rem(sp, RING)
    ka, qa = y + c * (z - y), z + c * (y - z)
    k_stride, q_stride = 1 + 7 * c, 8 - 7 * c

    def ring(pos, offset):
        return lax.rem(pos + (offset + RING), RING)

    def k_dev(offset):
        return (sp + (ring(ka, offset) - ka) * k_stride, tp)

    def q_dev(offset):
        return (sp + (ring(qa, offset) - qa) * q_stride, tp)

    def chip(offset):
        return lax.rem(x + offset, NX)

    def t_dev(xx, cc):
        return (sp, 2 * xx + cc)

    scopes = []
    A, L, Q, KV, O, ST, EP, EX, H, W, AT = (sent.at[i] for i in range(11))

    def phase(name):
        if scopes:
            scopes.pop().__exit__(None, None, None)
        if name:
            scopes.append(jax.named_scope(name))
            scopes[-1].__enter__()

    def remote(src, dst, send, recv, dev):
        return pltpu.make_async_remote_copy(
            src_ref=src, dst_ref=dst, send_sem=send, recv_sem=recv, device_id=dev, device_id_type=MESH
        )

    def push(src, dst, send, recv, dev):
        remote(src, dst, send, recv, dev).start()

    def arrived(bytes_of, recv):
        remote(bytes_of, bytes_of, A, recv, t_dev(x, 1 - c)).wait_recv()

    phase("loads")
    def load(i, *pairs):
        for src, dst in pairs:
            pltpu.make_async_copy(src, dst, load_sem.at[i]).start()

    def loaded(i, ref):
        pltpu.make_async_copy(ref, ref, load_sem.at[i]).wait()

    load(0, (act_hbm, act_all.at[tp]))
    load(1, (gain_hbm, gain))
    load(
        2,
        (qw_hbm, wt.at[pl.ds(0, 192), :]),
        (rw_hbm, wt.at[pl.ds(192, 64), :]),
        (lw_hbm, wt.at[pl.ds(256, 64), :]),
        (lw_hbm, wt.at[pl.ds(320, 64), :]),
    )
    load(
        3,
        (gw_hbm, wb.at[:, pl.ds(0, 128)]),
        (pw_hbm, wb.at[:, pl.ds(128, 128)]),
        (vw_hbm, wb.at[:, pl.ds(256, 128)]),
    )
    load(4, (lgain_hbm, lgain))
    load(5, (table_hbm, table))
    load(6, (ck_hbm, ck))
    load(7, (ew_hbm, ew))
    load(8, (oa_hbm, wa_all.at[tp]))
    load(9, (oc_hbm, wc))

    phase("barrier")
    barrier = pltpu.get_barrier_semaphore()
    partners = [(sp, lax.rem(tp + k, 8)) for k in range(1, 8)]
    partners += [q_dev(k) for k in range(1, 8)] + [k_dev(k) for k in (1, -1, 2, -2)]
    after, before = (lax.rem(sp + 1, 64), tp), (lax.rem(sp + 63, 64), tp)
    partners += [after, before]
    for dev in partners:
        pl.semaphore_signal(barrier, inc=1, device_id=dev, device_id_type=MESH)
    loaded(0, act_all.at[tp])
    pl.semaphore_wait(barrier, len(partners))

    phase("act_own")
    def rows_at(slot, ch, n):
        return act_all.at[slot, pl.ds(64 * ch, 64 * n), :]

    def a_push(slot, ch, n, recv, dev):
        push(rows_at(slot, ch, n), rows_at(slot, ch, n), A, a_recv.at[recv], dev)

    def a_wait(n, recv):
        arrived(act_all.at[0, pl.ds(0, 64 * n), :], a_recv.at[recv])

    up, down, mate = t_dev(chip(1), c), t_dev(chip(3), c), t_dev(x, 1 - c)
    for i in range(2):
        a_push(tp, i, 1, i, up)
        a_push(tp, 2 + i, 1, 3 + i, down)
    a_push(tp, 0, 4, 7, mate)
    a_push(tp, 2, 2, 2, up)
    a_push(tp, 0, 2, 5, down)
    loaded(1, gain)
    loaded(2, wt)
    loaded(3, wb)

    def project(slot, first):
        piece = act_all[slot].astype(F32)
        features = pl.ds(pl.multiple_of(slot * 256, 256), 256)
        scaled = (piece * gain[:, features]).astype(BF16)
        part = lax.dot_general(scaled, wt[:, features], (((1,), (1,)), ((), ())), preferred_element_type=F32)
        acc[...] = part if first else acc[...] + part
        part = jnp.dot(scaled, wb[features, :], preferred_element_type=F32)
        acc_b[...] = part if first else acc_b[...] + part
        squares = piece * piece
        return squares[:, 0:128] + squares[:, 128:256]

    squares = project(tp, True)
    phase("act_one")
    s_down, s_up, s_far = 2 * chip(3) + c, 2 * chip(1) + c, 2 * chip(2) + c
    other = 1 - 2 * c
    for i in range(2):
        a_wait(1, i)
        a_push(s_down, i, 1, 6, up)
        a_wait(1, 3 + i)
        a_push(s_up, 2 + i, 1, 6, down)
    a_wait(2, 2)
    a_push(s_down, 0, 4, 8, mate)
    a_wait(2, 5)
    a_push(s_up, 0, 4, 9, mate)
    a_wait(4, 7)
    squares += project(tp + other, False)
    squares += project(s_down, False)
    squares += project(s_up, False)
    a_wait(4, 8)
    squares += project(s_down + other, False)
    a_wait(4, 9)
    squares += project(s_up + other, False)
    phase("act_far")
    a_wait(4, 6)
    a_push(s_far, 0, 4, 10, mate)
    squares += project(s_far, False)
    a_wait(4, 10)
    squares += project(s_far + other, False)
    phase("latent_send")
    inv_rms = lax.rsqrt(jnp.sum(squares, axis=1, keepdims=True) / D + EPSILON)

    low = lane_iota(128) < 64
    latent_part = acc[:, 256:384] * inv_rms
    lat_all[tp] = jnp.where(low, latent_part[0:128], latent_part[128:256]).astype(BF16)

    def l_push(slot, recv, dev):
        push(lat_all.at[slot], lat_all.at[slot], L, l_recv.at[recv], dev)

    for i, dev in enumerate((t_dev(chip(2), c), up, down, mate)):
        l_push(tp, i, dev)

    phase("query")
    loaded(4, lgain)
    loaded(5, table)
    loaded(6, ck)
    loaded(7, ew)
    loaded(8, wa_all.at[tp])
    loaded(9, wc)
    scale = (NOPE + ROPE) ** (-0.5) * LOG2E
    q_all[qa, 0:256, :] = (acc[:, 0:128] * inv_rms * scale).astype(BF16)
    raw = acc[:, 128:256] * inv_rms
    even = lax.rem(lax.div(lane_iota(T), 16), 2) == 0
    tables = [table[pl.ds(sp * 4 + g, 1), :] + table[256:320, :] for g in range(4)]
    tables = jnp.concatenate(tables, axis=0)
    turned = jnp.where(even, pltpu.roll(raw, 112, 1), pltpu.roll(raw, 16, 1))
    rotated = raw * tables[:, 0:128] + turned * tables[:, 128:256]
    swapped = pltpu.roll(rotated, 64, 1)
    q_all[qa, 256:384, :] = (jnp.where(low, rotated[0:128], swapped[128:256]) * scale).astype(BF16)

    def spread(blocks, pos, rows, lead, stage, recv, dev):
        def move(offset, row, n, sem, to):
            part = blocks.at[ring(pos, offset), pl.ds(row, n), :]
            push(part, part, stage, recv.at[sem], dev(to))

        half, n = rows // 2, rows // 2 // lead

        def begin():
            for i in range(lead):
                move(0, i * n, n, i, 2)
                move(0, half + i * n, n, i, -2)
            move(0, 0, rows, lead + 1, 1)
            move(0, 0, rows, lead + 1, -1)
            move(0, half, half, lead, 2)
            move(0, 0, half, lead, -2)

        def onward_lead():
            for i in range(lead):
                arrived(blocks.at[0, pl.ds(0, 2 * n), :], recv.at[i])
                move(-2, i * n, n, lead + 3, 2)
                move(2, half + i * n, n, lead + 3, -2)
                move(-2, i * n, n, lead + 2, 1)
                move(2, half + i * n, n, lead + 2, -1)

        def onward_rest():
            arrived(blocks.at[0], recv.at[lead])
            move(-2, half, half, lead + 2, 1)
            move(2, 0, half, lead + 2, -1)

        def near():
            arrived(blocks.at[pl.ds(0, 2)], recv.at[lead + 1])

        def third():
            arrived(blocks.at[pl.ds(0, 2)], recv.at[lead + 2])

        def fourth():
            arrived(blocks.at[0], recv.at[lead + 3])

        return begin, onward_lead, onward_rest, near, third, fourth

    q_begin, q_onward_lead, q_onward_rest, q_near, q_third, q_fourth = spread(q_all, qa, Q_ROWS, 1, Q, q_recv, q_dev)
    k_begin, k_onward_lead, k_onward_rest, k_near, k_third, k_fourth = spread(kv_all, ka, KV_ROWS, 2, KV, kv_recv, k_dev)
    q_begin()

    def open_query(slot):
        paired = q_all[slot, 256:384, :].astype(F32)
        q_cat[slot, :, 0:128] = q_all[slot, 0:256, :]
        q_cat[slot, 0:128, 128:256] = jnp.where(low, paired, 0.0).astype(BF16)
        q_cat[slot, 128:256, 128:256] = jnp.where(low, pltpu.roll(paired, 64, 1), 0.0).astype(BF16)

    def open_keys(slot):
        paired = kv_all[slot, 256:384, :]
        k_cat[slot, :, 0:128] = kv_all[slot, 0:256, :]
        k_cat[slot, 0:128, 128:256] = paired
        k_cat[slot, 128:256, 128:256] = pltpu.roll(paired.astype(F32), 64, 1).astype(BF16)
        vt_all[slot, 0:128, :] = jnp.transpose(kv_all[slot, 384:640, :].astype(F32)).astype(BF16)

    phase("halo")
    pre_mix = (acc_b[:, 128:256] * inv_rms) * (acc_b[:, 256:384] * inv_rms)
    pre_mix = pre_mix.astype(BF16).astype(F32)
    halo_out[0] = pre_mix[0:8]
    halo_out[1] = pre_mix[248:256]
    push(halo_out.at[0], halo_in.at[1], H, h_recv.at[0], before)
    push(halo_out.at[1], halo_in.at[0], H, h_recv.at[0], after)
    gate = acc_b[:, 0:128] * inv_rms

    phase("latent_wait")
    def w_push(slot, h, n, recv, dev):
        part = wa_all.at[slot, pl.ds(64 * h, 64 * n), :]
        push(part, part, W, w_recv.at[recv], dev)

    def w_start():
        w_push(tp, 0, 1, 0, up)
        w_push(tp, 1, 1, 1, down)
        w_push(tp, 0, 2, 4, mate)
        w_push(tp, 1, 1, 2, up)
        w_push(tp, 0, 1, 2, down)

    def w_onward():
        arrived(wa_all.at[0, pl.ds(0, 64), :], w_recv.at[0])
        w_push(s_down, 0, 1, 3, up)
        arrived(wa_all.at[0, pl.ds(0, 64), :], w_recv.at[1])
        w_push(s_up, 1, 1, 3, down)

    def w_near_to_mate():
        arrived(wa_all.at[0], w_recv.at[2])
        w_push(s_down, 0, 2, 4, mate)
        w_push(s_up, 0, 2, 4, mate)

    def w_far_to_mate():
        arrived(wa_all.at[0], w_recv.at[3])
        w_push(s_far, 0, 2, 4, mate)

    kv_rope = jnp.where(low, swapped[0:128], rotated[128:256]).astype(BF16)
    kv_all[ka, 256:384, :] = kv_rope
    open_query(qa)
    stats[:, 0:1, :] = jnp.full((8, 1, T), LOW, F32)
    stats[:, 1:8, :] = jnp.zeros((8, 7, T), F32)
    o_acc[...] = jnp.zeros_like(o_acc)
    ones = lax.broadcasted_iota(jnp.int32, (8, V_ROWS - 128, T), 1) == 0
    vt_all[:, 128:V_ROWS, :] = jnp.where(ones, 1.0, 0.0).astype(BF16)
    phase("latent_x")
    for recv, slot in ((1, s_down), (2, s_up), (0, s_far)):
        arrived(lat_all.at[0], l_recv.at[recv])
        l_push(slot, 3, mate)
    phase("q2")
    q_onward_lead()
    w_start()
    phase("latent_mate")
    arrived(lat_all.at[pl.ds(0, 4)], l_recv.at[3])

    def pair(j):
        a, b = lat_all[2 * j].astype(F32), lat_all[2 * j + 1].astype(F32)
        return jnp.concatenate(
            [jnp.where(low, a, pltpu.roll(b, 64, 1)), jnp.where(low, pltpu.roll(a, 64, 1), b)], axis=0
        )

    phase("expand")
    parts = jnp.concatenate([pair(j) for j in range(4)], axis=1)
    latent_inv = lax.rsqrt(jnp.mean(parts * parts, axis=1, keepdims=True) + EPSILON)
    latent = (parts * latent_inv * lgain[...]).astype(BF16)
    expanded = jnp.dot(latent, ew[...], preferred_element_type=F32).astype(BF16)
    kv_all[ka, 0:256, :] = expanded[:, 0:128]
    kv_all[ka, 384:640, :] = expanded[:, 128:256]
    k_begin()
    phase("q2_rest")
    q_onward_rest()
    phase("conv")
    arrived(halo_in, h_recv.at[0])
    row = lax.broadcasted_iota(jnp.int32, (T, 128), 0)
    first = jnp.where(sp > 0, halo_in[0, 7:8, :], 0.0)
    last = jnp.where(sp < 63, halo_in[1, 0:1, :], 0.0)
    shifted_down = jnp.where(row == 0, first, pltpu.roll(pre_mix, 1, 0))
    shifted_up = jnp.where(row == T - 1, last, pltpu.roll(pre_mix, T - 1, 0))
    taps = ck[...].astype(F32)
    convolved = taps[0:1] * shifted_down + taps[1:2] * pre_mix + taps[2:3] * shifted_up
    conv_mixed[...] = (gate * convolved).astype(BF16)
    open_keys(ka)

    phase("conv_out")

    def rows_of(xx, cc):
        return pl.ds(pl.multiple_of((2 * xx + cc) * 32, 32), 32)

    order = [chip(2), chip(1), chip(3), x]
    for_mate = jnp.concatenate([conv_mixed[rows_of(xx, 1 - c), :] for xx in order], axis=0)
    for n in range(4):
        cols = slice(512 * n, 512 * n + 512)
        part = jnp.dot(for_mate, wc[:, cols], preferred_element_type=F32).astype(BF16)
        for j in range(4):
            e_psend[j, :, cols] = part[32 * j : 32 * j + 32]
    for j in range(4):
        push(e_psend.at[j], e_precv.at[j], EP, ep_recv.at[j], mate)
    for_own = jnp.concatenate([conv_mixed[rows_of(xx, c), :] for xx in order], axis=0)
    for n in range(4):
        cols = slice(512 * n, 512 * n + 512)
        part = jnp.dot(for_own, wc[:, cols], preferred_element_type=F32)
        for j in range(4):
            e_own[j, :, cols] = part[32 * j : 32 * j + 32]

    def key_blocks(ks, qs):
        n = len(ks) * T
        keys = jnp.concatenate([k_cat[k] for k in ks], axis=0)
        values = jnp.concatenate([vt_all[k] for k in ks], axis=1)
        for i, q in enumerate(qs):
            s_buf[i, 0:n] = lax.dot_general(keys, q_cat[q], (((1,), (1,)), ((), ())), preferred_element_type=F32)
        for i, q in enumerate(qs):
            scores = s_buf[i, 0:n]
            old_max = stats[q, 0:1, :]
            new_max = jnp.maximum(old_max, jnp.max(scores, axis=0, keepdims=True))
            r_buf[i, 0:1, :] = jnp.exp2(old_max - new_max)
            stats[q, 0:1, :] = new_max
            w_buf[i, 0:n] = jnp.exp2(scores - new_max).astype(BF16)
        for i, q in enumerate(qs):
            yield o_acc[q] * r_buf[i, 0:1, :] + jnp.dot(values, w_buf[i, 0:n], preferred_element_type=F32)

    def attend(ks, qs):
        for q, out in zip(qs, key_blocks(ks, qs)):
            o_acc[q] = out

    def d_push(offset):
        slot = ring(qa, offset)
        push(o_send.at[slot], o_recv.at[qa], O, d_recv.at[0], q_dev(offset))
        push(stats.at[slot], st_recv.at[qa], ST, d_recv.at[1], q_dev(offset))

    def key_step(step, _):
        for s in (1, 2):

            @pl.when(step == s)
            def _(s=s):
                if s == 1:
                    k_near()
                if s == 2:
                    k_onward_rest()
                    w_onward()
                    conv_onward()
                for d in (s, -s):
                    open_keys(ring(ka, d))

        ks = (lax.rem(ka + step, RING), lax.rem(ka - step + RING, RING))
        attend(ks, range(8))
        return 0

    def conv_onward():
        for j in range(3):
            push(e_xsend.at[j], e_xrecv.at[j], EX, ex_recv.at[0], t_dev(order[j], c))

    phase("q_rest")
    q_near()
    for offset in (1, -1, 2, -2):
        open_query(ring(qa, offset))
    own = (ka,)
    phase("own_keys")
    attend(own, [ring(qa, offset) for offset in (0, 1, -1, 2, -2)])
    phase("k_lead")
    k_onward_lead()
    phase("q3")
    q_third()
    for offset in (3, -3):
        open_query(ring(qa, offset))
    phase("q4")
    q_fourth()
    open_query(ring(qa, 4))

    phase("own_rest")
    attend(own, [ring(qa, offset) for offset in (3, -3, 4)])
    phase("conv_mate")
    for j in range(4):
        arrived(e_precv.at[j], ep_recv.at[j])
        both = e_own[j] + e_precv[j].astype(F32)
        if j < 3:
            e_xsend[j] = both.astype(BF16)
        else:
            e_own[j] = both
    phase("keys")
    lax.fori_loop(1, 3, key_step, 0)
    phase("k4")
    k_fourth()
    open_keys(ring(ka, 4))
    attend((ring(ka, 4),), range(8))
    phase("k3")
    k_third()
    for d in (3, -3):
        open_keys(ring(ka, d))
    phase("last_keys")
    for offsets in ((4, 3, 5), (2, 6), (1, 7, 0)):
        qs = [ring(qa, offset) for offset in offsets]
        for offset, q, out in zip(offsets, qs, key_blocks((ring(ka, 3), ring(ka, -3)), qs)):
            stats[q, 1:2, :] = out[128:129]
            if offset:
                o_send[q] = out[0:128].astype(BF16)
            else:
                o_acc[qa] = out
        for offset in offsets:
            if offset:
                d_push(offset)
    phase("w_near")
    w_near_to_mate()
    phase("w_far")
    w_far_to_mate()
    phase("d_wait")
    arrived(st_recv.at[pl.ds(0, 7)], d_recv.at[1])
    arrived(o_recv.at[pl.ds(0, 7)], d_recv.at[0])
    phase("merge")
    whole_max = stats[qa, 0:1, :]
    for offset in range(1, 8):
        whole_max = jnp.maximum(whole_max, st_recv[ring(qa, offset), 0:1, :])
    weight = jnp.exp2(stats[qa, 0:1, :] - whole_max)
    whole_sum = stats[qa, 1:2, :] * weight
    whole_out = o_acc[qa, 0:128, :] * weight
    for offset in range(1, 8):
        slot = ring(qa, offset)
        weight = jnp.exp2(st_recv[slot, 0:1, :] - whole_max)
        whole_sum += st_recv[slot, 1:2, :] * weight
        whole_out += o_recv[slot].astype(F32) * weight
    lws_ref[...] = whole_max * (1.0 / LOG2E) + jnp.log(whole_sum)
    attended[...] = jnp.transpose(whole_out / whole_sum).astype(BF16)

    phase("heads")
    for k in range(1, 8):
        peer = lax.rem(tp + k, 8)
        rows = pl.ds(pl.multiple_of(peer * 32, 32), 32)
        push(attended.at[rows, :], heads.at[tp], AT, at_recv.at[0], (sp, peer))
    heads[tp] = attended[pl.ds(pl.multiple_of(tp * 32, 32), 32), :]
    phase("conv_sum")
    arrived(e_xrecv, ex_recv.at[0])
    e_own[3] = e_own[3] + e_xrecv[0].astype(F32) + e_xrecv[1].astype(F32) + e_xrecv[2].astype(F32)
    phase("w_wait")
    arrived(wa_all.at[pl.ds(0, 4)], w_recv.at[4])
    phase("heads_wait")
    arrived(heads.at[pl.ds(0, 7)], at_recv.at[0])
    phase("out")
    side_by_side = jnp.concatenate([heads[j] for j in range(8)], axis=1)
    for n in range(4):
        cols = slice(512 * n, 512 * n + 512)
        weights = wa_all[:, :, cols].reshape(1024, 512)
        out = jnp.dot(side_by_side, weights, preferred_element_type=F32)
        mixed_ref[:, cols] = (out + e_own[3, :, cols]).astype(BF16)
    phase("send_wait")
    for ref, send in (
        (act_all.at[pl.ds(0, 7)], A),
        (lat_all.at[pl.ds(0, 7)], L),
        (q_all.at[pl.ds(0, 7)], Q),
        (kv_all.at[pl.ds(0, 7)], KV),
        (o_send.at[pl.ds(0, 7)], O),
        (stats.at[pl.ds(0, 7)], ST),
        (e_psend, EP),
        (e_xsend, EX),
        (halo_out, H),
        (wa_all.at[pl.ds(0, 7)], W),
        (heads.at[pl.ds(0, 7)], AT),
    ):
        remote(ref, ref, send, d_recv.at[0], mate).wait_send()
    phase(None)


def body(
    activations, norm_gain, query_weight, latent_weight, rope_key_weight, latent_gain, expand_weight,
    gate_weight, pre_weight, value_weight, conv_kernel, output_attend, output_conv,
):
    dma = pltpu.SemaphoreType.DMA
    vmem = pltpu.VMEM
    return pl.pallas_call(
        kernel,
        out_shape=(vmem((32, D), BF16), vmem((1, T), F32)),
        in_specs=[pl.BlockSpec(memory_space=pl.ANY)] * 14,
        out_specs=(pl.BlockSpec(memory_space=vmem), pl.BlockSpec(memory_space=vmem)),
        scratch_shapes=[
            vmem((8, T, 256), BF16),
            vmem((1, D), F32),
            vmem((1, 512), F32),
            vmem((512, 256), BF16),
            vmem((384, D), BF16),
            vmem((D, 384), BF16),
            vmem((3, 128), BF16),
            vmem((8, 128, D), BF16),
            vmem((128, D), BF16),
            vmem((320, 256), F32),
            vmem((T, 384), F32),
            vmem((T, 384), F32),
            vmem((8, 128, 128), BF16),
            vmem((8, Q_ROWS, 128), BF16),
            vmem((8, T, 256), BF16),
            vmem((8, KV_ROWS, 128), BF16),
            vmem((8, T, 256), BF16),
            vmem((8, V_ROWS, T), BF16),
            vmem((8, 2 * T, T), F32),
            vmem((8, 2 * T, T), BF16),
            vmem((8, 8, T), F32),
            vmem((8, 8, T), F32),
            vmem((8, V_ROWS, T), F32),
            vmem((8, 128, T), BF16),
            vmem((8, 128, T), BF16),
            vmem((8, 8, T), F32),
            vmem((2, 8, 128), F32),
            vmem((2, 8, 128), F32),
            vmem((T, 128), BF16),
            vmem((T, 128), BF16),
            vmem((8, 32, 128), BF16),
            vmem((4, 32, D), BF16),
            vmem((4, 32, D), BF16),
            vmem((4, 32, D), F32),
            vmem((3, 32, D), BF16),
            vmem((3, 32, D), BF16),
            dma((10,)),
            dma((11,)),
            dma((11,)),
            dma((4,)),
            dma((5,)),
            dma((6,)),
            dma((2,)),
            dma((1,)),
            dma((4,)),
            dma((1,)),
            dma((5,)),
            dma((1,)),
        ],
        compiler_params=pltpu.CompilerParams(collective_id=0, has_side_effects=True),
    )(
        activations, norm_gain.reshape(1, D), query_weight.T, latent_weight.T, rope_key_weight.T,
        latent_gain.reshape(1, 512), expand_weight, gate_weight, pre_weight, value_weight, conv_kernel,
        output_attend, output_conv, jnp.asarray(rotation_tables()),
    )


def solution(mesh):
    return jax.shard_map(
        body,
        mesh=mesh,
        in_specs=(
            P("sp", "tp"),
            P(),
            P(None, "tp"),
            P(None, "tp"),
            P(),
            P(),
            P(None, "tp"),
            P(None, "tp"),
            P(None, "tp"),
            P(None, "tp"),
            P(None, "tp"),
            P("tp", None),
            P("tp", None),
        ),
        out_specs=(P(("sp", "tp"), None), P("tp", "sp")),
        check_vma=False,
    )
```

```python
import functools

import jax
import jax.numpy as jnp
import numpy as np
from jax import lax
from jax.experimental import pallas as pl
from jax.experimental.pallas import tpu as pltpu
from jax.sharding import PartitionSpec as P

MESH = pl.DeviceIdType.MESH
F32 = jnp.float32
BF16 = jnp.bfloat16

D = 2048
NOPE = 128
ROPE = 64
GRID_W = 64
EPSILON = 1e-06
ROPE_BASE = 10000.0
RING = 8
NX = 4
T = 256
Q_ROWS = 384
KV_ROWS, ROPE_ROWS = 512, 128
V_ROWS = 144
LOW = -3.0e38
LOG2E = 1.4426950408889634


def rotation_tables():
    inverse = (np.float32(ROPE_BASE) ** (-np.arange(16, dtype=np.float32) / np.float32(16))).astype(np.float32)
    quarter = np.arange(128) // 16 % 4
    freq = inverse[np.arange(128) % 16]
    sign = np.where(quarter % 2 == 0, -1.0, 1.0)

    def table(count, mask):
        angle = (np.arange(count, dtype=np.float32)[:, None] * freq[None, :]).astype(np.float32)
        angle = angle.astype(np.float64)
        return np.concatenate([np.cos(angle) * mask, np.sin(angle) * sign * mask], axis=1).astype(np.float32)

    return np.concatenate([table(256, quarter < 2), table(GRID_W, quarter >= 2)])


def lane_iota(rows):
    return lax.broadcasted_iota(jnp.int32, (rows, 128), 1)


def kernel(
    act_hbm, gain_hbm, qw_hbm, lw_hbm, rw_hbm, lgain_hbm, ew_hbm, gw_hbm, pw_hbm, vw_hbm, ck_hbm, oa_hbm, oc_hbm,
    table_hbm,
    mixed_ref, lws_ref,
    act_all, gain, lgain, ew, wt, wb, ck, wa_all, wc, table, acc, acc_b, lat_all,
    q_all, q_cat, kv_all, rope_all, k_cat, vt_all, s_buf, w_buf, r_buf, stats, o_acc, o_send, o_recv, st_recv,
    halo_out, halo_in, conv_mixed, attended, heads, e_psend, e_precv, e_own, e_xsend, e_xrecv,
    load_sem, sent, a_recv, l_recv, q_recv, kv_recv, r_recv, d_recv, h_recv, ep_recv, ex_recv, w_recv, at_recv,
):
    sp = lax.axis_index("sp")
    tp = lax.axis_index("tp")
    x, c = lax.div(tp, 2), lax.rem(tp, 2)
    z, y = lax.div(sp, RING), lax.rem(sp, RING)
    ka, qa = y + c * (z - y), z + c * (y - z)
    k_stride, q_stride = 1 + 7 * c, 8 - 7 * c

    def ring(pos, offset):
        return lax.rem(pos + (offset + RING), RING)

    def k_dev(offset):
        return (sp + (ring(ka, offset) - ka) * k_stride, tp)

    def q_dev(offset):
        return (sp + (ring(qa, offset) - qa) * q_stride, tp)

    def chip(offset):
        return lax.rem(x + offset, NX)

    def t_dev(xx, cc):
        return (sp, 2 * xx + cc)

    scopes = []
    A, L, Q, KV, O, ST, EP, EX, H, W, AT, R = (sent.at[i] for i in range(12))

    def phase(name):
        if scopes:
            scopes.pop().__exit__(None, None, None)
        if name:
            scopes.append(jax.named_scope(name))
            scopes[-1].__enter__()

    def remote(src, dst, send, recv, dev):
        return pltpu.make_async_remote_copy(
            src_ref=src, dst_ref=dst, send_sem=send, recv_sem=recv, device_id=dev, device_id_type=MESH
        )

    def push(src, dst, send, recv, dev):
        remote(src, dst, send, recv, dev).start()

    def arrived(bytes_of, recv):
        remote(bytes_of, bytes_of, A, recv, t_dev(x, 1 - c)).wait_recv()

    phase("loads")
    def load(i, *pairs):
        for src, dst in pairs:
            pltpu.make_async_copy(src, dst, load_sem.at[i]).start()

    def loaded(i, ref):
        pltpu.make_async_copy(ref, ref, load_sem.at[i]).wait()

    load(0, (act_hbm, act_all.at[tp]))
    load(1, (gain_hbm, gain))
    load(
        2,
        (qw_hbm, wt.at[pl.ds(0, 192), :]),
        (rw_hbm, wt.at[pl.ds(192, 64), :]),
        (lw_hbm, wt.at[pl.ds(256, 64), :]),
        (lw_hbm, wt.at[pl.ds(320, 64), :]),
    )
    load(
        3,
        (gw_hbm, wb.at[:, pl.ds(0, 128)]),
        (pw_hbm, wb.at[:, pl.ds(128, 128)]),
        (vw_hbm, wb.at[:, pl.ds(256, 128)]),
    )
    load(4, (lgain_hbm, lgain))
    load(5, (table_hbm, table))
    load(6, (ck_hbm, ck))
    load(7, (ew_hbm, ew))
    load(8, (oa_hbm, wa_all.at[tp]))
    load(9, (oc_hbm, wc))

    phase("barrier")
    barrier = pltpu.get_barrier_semaphore()
    partners = [(sp, lax.rem(tp + k, 8)) for k in range(1, 8)]
    partners += [dev(k) for dev in (q_dev, k_dev) for k in (1, -1, 2, -2)]
    after, before = (lax.rem(sp + 1, 64), tp), (lax.rem(sp + 63, 64), tp)
    partners += [after, before]
    for dev in partners:
        pl.semaphore_signal(barrier, inc=1, device_id=dev, device_id_type=MESH)
    loaded(0, act_all.at[tp])
    pl.semaphore_wait(barrier, len(partners))

    phase("act_own")
    def rows_at(slot, ch, n):
        return act_all.at[slot, pl.ds(64 * ch, 64 * n), :]

    def a_push(slot, ch, n, recv, dev):
        push(rows_at(slot, ch, n), rows_at(slot, ch, n), A, a_recv.at[recv], dev)

    def a_wait(n, recv):
        arrived(act_all.at[0, pl.ds(0, 64 * n), :], a_recv.at[recv])

    up, down, mate = t_dev(chip(1), c), t_dev(chip(3), c), t_dev(x, 1 - c)
    for i in range(2):
        a_push(tp, i, 1, i, up)
        a_push(tp, 2 + i, 1, 3 + i, down)
    a_push(tp, 0, 4, 7, mate)
    a_push(tp, 2, 2, 2, up)
    a_push(tp, 0, 2, 5, down)
    loaded(1, gain)
    loaded(2, wt)
    loaded(3, wb)

    def project(slot, first):
        piece = act_all[slot].astype(F32)
        features = pl.ds(pl.multiple_of(slot * 256, 256), 256)
        scaled = (piece * gain[:, features]).astype(BF16)
        part = lax.dot_general(scaled, wt[:, features], (((1,), (1,)), ((), ())), preferred_element_type=F32)
        acc[...] = part if first else acc[...] + part
        part = jnp.dot(scaled, wb[features, :], preferred_element_type=F32)
        acc_b[...] = part if first else acc_b[...] + part
        squares = piece * piece
        return squares[:, 0:128] + squares[:, 128:256]

    squares = project(tp, True)
    phase("act_one")
    s_down, s_up, s_far = 2 * chip(3) + c, 2 * chip(1) + c, 2 * chip(2) + c
    other = 1 - 2 * c
    for i in range(2):
        a_wait(1, i)
        a_push(s_down, i, 1, 6, up)
        a_wait(1, 3 + i)
        a_push(s_up, 2 + i, 1, 6, down)
    a_wait(2, 2)
    a_push(s_down, 0, 4, 8, mate)
    a_wait(2, 5)
    a_push(s_up, 0, 4, 9, mate)
    a_wait(4, 7)
    squares += project(tp + other, False)
    squares += project(s_down, False)
    squares += project(s_up, False)
    a_wait(4, 8)
    squares += project(s_down + other, False)
    a_wait(4, 9)
    squares += project(s_up + other, False)
    phase("act_far")
    a_wait(4, 6)
    a_push(s_far, 0, 4, 10, mate)
    squares += project(s_far, False)
    a_wait(4, 10)
    squares += project(s_far + other, False)
    phase("latent_send")
    inv_rms = lax.rsqrt(jnp.sum(squares, axis=1, keepdims=True) / D + EPSILON)

    def w_push(slot, h, n, recv, dev):
        part = wa_all.at[slot, pl.ds(64 * h, 64 * n), :]
        push(part, part, W, w_recv.at[recv], dev)

    def w_start():
        w_push(tp, 0, 1, 0, up)
        w_push(tp, 1, 1, 1, down)
        w_push(tp, 0, 2, 4, mate)
        w_push(tp, 1, 1, 2, up)
        w_push(tp, 0, 1, 2, down)

    def w_onward():
        arrived(wa_all.at[0, pl.ds(0, 64), :], w_recv.at[0])
        w_push(s_down, 0, 1, 3, up)
        arrived(wa_all.at[0, pl.ds(0, 64), :], w_recv.at[1])
        w_push(s_up, 1, 1, 3, down)

    def w_near_to_mate():
        arrived(wa_all.at[0], w_recv.at[2])
        w_push(s_down, 0, 2, 4, mate)
        w_push(s_up, 0, 2, 4, mate)

    def w_far_to_mate():
        arrived(wa_all.at[0], w_recv.at[3])
        w_push(s_far, 0, 2, 4, mate)

    low = lane_iota(128) < 64
    latent_part = acc[:, 256:384] * inv_rms
    lat_all[tp] = jnp.where(low, latent_part[0:128], latent_part[128:256]).astype(BF16)

    def l_push(slot, recv, dev):
        push(lat_all.at[slot], lat_all.at[slot], L, l_recv.at[recv], dev)

    for i, dev in enumerate((t_dev(chip(2), c), up, down, mate)):
        l_push(tp, i, dev)
    loaded(8, wa_all.at[tp])
    w_start()

    phase("query")
    loaded(4, lgain)
    loaded(5, table)
    loaded(6, ck)
    loaded(7, ew)
    loaded(9, wc)
    scale = (NOPE + ROPE) ** (-0.5) * LOG2E
    q_all[qa, 0:256, :] = (acc[:, 0:128] * inv_rms * scale).astype(BF16)
    raw = acc[:, 128:256] * inv_rms
    even = lax.rem(lax.div(lane_iota(T), 16), 2) == 0
    tables = [table[pl.ds(sp * 4 + g, 1), :] + table[256:320, :] for g in range(4)]
    tables = jnp.concatenate(tables, axis=0)
    turned = jnp.where(even, pltpu.roll(raw, 112, 1), pltpu.roll(raw, 16, 1))
    rotated = raw * tables[:, 0:128] + turned * tables[:, 128:256]
    swapped = pltpu.roll(rotated, 64, 1)
    q_all[qa, 256:384, :] = (jnp.where(low, rotated[0:128], swapped[128:256]) * scale).astype(BF16)

    def spread(blocks, pos, rows, lead, stage, recv, dev):
        def move(offset, row, n, sem, to):
            part = blocks.at[ring(pos, offset), pl.ds(row, n), :]
            push(part, part, stage, recv.at[sem], dev(to))

        half, n = rows // 2, rows // 2 // lead

        def begin():
            for i in range(lead):
                move(0, i * n, n, i, 2)
                move(0, half + i * n, n, i, -2)
            move(0, 0, rows, lead + 1, 1)
            move(0, 0, rows, lead + 1, -1)
            move(0, half, half, lead, 2)
            move(0, 0, half, lead, -2)

        def onward_lead():
            for i in range(lead):
                arrived(blocks.at[0, pl.ds(0, 2 * n), :], recv.at[i])
                move(-2, i * n, n, lead + 3, 2)
                move(2, half + i * n, n, lead + 3, -2)
                move(-2, i * n, n, lead + 2, 1)
                move(2, half + i * n, n, lead + 2, -1)

        def onward_rest():
            arrived(blocks.at[0], recv.at[lead])
            move(-2, half, half, lead + 2, 1)
            move(2, 0, half, lead + 2, -1)

        def near():
            arrived(blocks.at[pl.ds(0, 2)], recv.at[lead + 1])

        def third():
            arrived(blocks.at[pl.ds(0, 2)], recv.at[lead + 2])

        def fourth():
            arrived(blocks.at[0], recv.at[lead + 3])

        return begin, onward_lead, onward_rest, near, third, fourth

    q_begin, q_onward_lead, q_onward_rest, q_near, q_third, q_fourth = spread(q_all, qa, Q_ROWS, 1, Q, q_recv, q_dev)
    r_begin, r_onward_lead, r_onward_rest, r_near, r_third, r_fourth = spread(rope_all, ka, ROPE_ROWS, 1, R, r_recv, k_dev)
    k_begin, k_onward_lead, k_onward_rest, k_near, k_third, k_fourth = spread(kv_all, ka, KV_ROWS, 2, KV, kv_recv, k_dev)
    q_begin()
    rope_all[ka] = jnp.where(low, swapped[0:128], rotated[128:256]).astype(BF16)

    def open_query(slot):
        paired = q_all[slot, 256:384, :].astype(F32)
        q_cat[slot, :, 0:128] = q_all[slot, 0:256, :]
        q_cat[slot, 0:128, 128:256] = jnp.where(low, paired, 0.0).astype(BF16)
        q_cat[slot, 128:256, 128:256] = jnp.where(low, pltpu.roll(paired, 64, 1), 0.0).astype(BF16)

    def open_keys(slot):
        paired = rope_all[slot]
        k_cat[slot, :, 0:128] = kv_all[slot, 0:256, :]
        k_cat[slot, 0:128, 128:256] = paired
        k_cat[slot, 128:256, 128:256] = pltpu.roll(paired.astype(F32), 64, 1).astype(BF16)
        vt_all[slot, 0:128, :] = jnp.transpose(kv_all[slot, 256:512, :].astype(F32)).astype(BF16)

    phase("halo")
    pre_mix = (acc_b[:, 128:256] * inv_rms) * (acc_b[:, 256:384] * inv_rms)
    pre_mix = pre_mix.astype(BF16).astype(F32)
    halo_out[0] = pre_mix[0:8]
    halo_out[1] = pre_mix[248:256]
    push(halo_out.at[0], halo_in.at[1], H, h_recv.at[0], before)
    push(halo_out.at[1], halo_in.at[0], H, h_recv.at[0], after)
    gate = acc_b[:, 0:128] * inv_rms

    phase("latent_wait")
    open_query(qa)
    stats[:, 0:1, :] = jnp.full((8, 1, T), LOW, F32)
    stats[:, 1:8, :] = jnp.zeros((8, 7, T), F32)
    o_acc[...] = jnp.zeros_like(o_acc)
    ones = lax.broadcasted_iota(jnp.int32, (8, V_ROWS - 128, T), 1) == 0
    vt_all[:, 128:V_ROWS, :] = jnp.where(ones, 1.0, 0.0).astype(BF16)
    phase("latent_x")
    for recv, slot in ((1, s_down), (2, s_up), (0, s_far)):
        arrived(lat_all.at[0], l_recv.at[recv])
        l_push(slot, 3, mate)
    r_begin()
    phase("q2")
    q_onward_lead()
    phase("latent_mate")
    arrived(lat_all.at[pl.ds(0, 4)], l_recv.at[3])

    def pair(j):
        a, b = lat_all[2 * j].astype(F32), lat_all[2 * j + 1].astype(F32)
        return jnp.concatenate(
            [jnp.where(low, a, pltpu.roll(b, 64, 1)), jnp.where(low, pltpu.roll(a, 64, 1), b)], axis=0
        )

    phase("expand")
    parts = jnp.concatenate([pair(j) for j in range(4)], axis=1)
    latent_inv = lax.rsqrt(jnp.mean(parts * parts, axis=1, keepdims=True) + EPSILON)
    latent = (parts * latent_inv * lgain[...]).astype(BF16)
    expanded = jnp.dot(latent, ew[...], preferred_element_type=F32).astype(BF16)
    kv_all[ka, 0:256, :] = expanded[:, 0:128]
    kv_all[ka, 256:512, :] = expanded[:, 128:256]
    k_begin()
    phase("q2_rest")
    q_onward_rest()
    phase("conv")
    arrived(halo_in, h_recv.at[0])
    row = lax.broadcasted_iota(jnp.int32, (T, 128), 0)
    first = jnp.where(sp > 0, halo_in[0, 7:8, :], 0.0)
    last = jnp.where(sp < 63, halo_in[1, 0:1, :], 0.0)
    shifted_down = jnp.where(row == 0, first, pltpu.roll(pre_mix, 1, 0))
    shifted_up = jnp.where(row == T - 1, last, pltpu.roll(pre_mix, T - 1, 0))
    taps = ck[...].astype(F32)
    convolved = taps[0:1] * shifted_down + taps[1:2] * pre_mix + taps[2:3] * shifted_up
    conv_mixed[...] = (gate * convolved).astype(BF16)
    open_keys(ka)

    phase("conv_out")

    def rows_of(xx, cc):
        return pl.ds(pl.multiple_of((2 * xx + cc) * 32, 32), 32)

    order = [chip(2), chip(1), chip(3), x]
    for_mate = jnp.concatenate([conv_mixed[rows_of(xx, 1 - c), :] for xx in order], axis=0)
    for n in range(4):
        cols = slice(512 * n, 512 * n + 512)
        part = jnp.dot(for_mate, wc[:, cols], preferred_element_type=F32).astype(BF16)
        for j in range(4):
            e_psend[j, :, cols] = part[32 * j : 32 * j + 32]
    for j in range(4):
        push(e_psend.at[j], e_precv.at[j], EP, ep_recv.at[j], mate)
    for_own = jnp.concatenate([conv_mixed[rows_of(xx, c), :] for xx in order], axis=0)
    for n in range(4):
        cols = slice(512 * n, 512 * n + 512)
        part = jnp.dot(for_own, wc[:, cols], preferred_element_type=F32)
        for j in range(4):
            e_own[j, :, cols] = part[32 * j : 32 * j + 32]

    def key_blocks(ks, qs):
        n = len(ks) * T
        keys = jnp.concatenate([k_cat[k] for k in ks], axis=0)
        values = jnp.concatenate([vt_all[k] for k in ks], axis=1)
        for i, q in enumerate(qs):
            s_buf[i, 0:n] = lax.dot_general(keys, q_cat[q], (((1,), (1,)), ((), ())), preferred_element_type=F32)
        for i, q in enumerate(qs):
            scores = s_buf[i, 0:n]
            old_max = stats[q, 0:1, :]
            new_max = jnp.maximum(old_max, jnp.max(scores, axis=0, keepdims=True))
            r_buf[i, 0:1, :] = jnp.exp2(old_max - new_max)
            stats[q, 0:1, :] = new_max
            w_buf[i, 0:n] = jnp.exp2(scores - new_max).astype(BF16)
        for i, q in enumerate(qs):
            yield o_acc[q] * r_buf[i, 0:1, :] + jnp.dot(values, w_buf[i, 0:n], preferred_element_type=F32)

    def attend(ks, qs):
        for q, out in zip(qs, key_blocks(ks, qs)):
            o_acc[q] = out

    def d_push(offset):
        slot = ring(qa, offset)
        push(o_send.at[slot], o_recv.at[qa], O, d_recv.at[0], q_dev(offset))
        push(stats.at[slot], st_recv.at[qa], ST, d_recv.at[1], q_dev(offset))

    def key_step(step, _):
        for s in (1, 2):

            @pl.when(step == s)
            def _(s=s):
                if s == 1:
                    r_near()
                    k_near()
                if s == 2:
                    k_onward_rest()
                for d in (s, -s):
                    open_keys(ring(ka, d))

        ks = (lax.rem(ka + step, RING), lax.rem(ka - step + RING, RING))
        attend(ks, range(8))
        return 0

    def conv_onward():
        for j in range(3):
            push(e_xsend.at[j], e_xrecv.at[j], EX, ex_recv.at[0], t_dev(order[j], c))

    phase("q_rest")
    q_near()
    for offset in (1, -1, 2, -2):
        open_query(ring(qa, offset))
    own = (ka,)
    phase("own_keys")
    attend(own, [ring(qa, offset) for offset in (0, 1, -1, 2, -2)])
    phase("rope_onward")
    r_onward_lead()
    r_onward_rest()
    phase("k_lead")
    k_onward_lead()
    phase("q3")
    q_third()
    for offset in (3, -3):
        open_query(ring(qa, offset))
    phase("q4")
    q_fourth()
    open_query(ring(qa, 4))

    phase("w_onward")
    w_onward()
    phase("own_rest")
    attend(own, [ring(qa, offset) for offset in (3, -3, 4)])
    phase("conv_mate")
    for j in range(4):
        arrived(e_precv.at[j], ep_recv.at[j])
        both = e_own[j] + e_precv[j].astype(F32)
        if j < 3:
            e_xsend[j] = both.astype(BF16)
        else:
            e_own[j] = both
    conv_onward()
    phase("keys")
    lax.fori_loop(1, 3, key_step, 0)
    phase("k4")
    r_fourth()
    k_fourth()
    open_keys(ring(ka, 4))
    attend((ring(ka, 4),), range(8))
    phase("k3")
    r_third()
    k_third()
    for d in (3, -3):
        open_keys(ring(ka, d))
    phase("last_keys")
    for offsets in ((4, 3, 5), (2, 6), (1, 7, 0)):
        qs = [ring(qa, offset) for offset in offsets]
        for offset, q, out in zip(offsets, qs, key_blocks((ring(ka, 3), ring(ka, -3)), qs)):
            stats[q, 1:2, :] = out[128:129]
            if offset:
                o_send[q] = out[0:128].astype(BF16)
            else:
                o_acc[qa] = out
        for offset in offsets:
            if offset:
                d_push(offset)
    phase("w_near")
    w_near_to_mate()
    phase("w_far")
    w_far_to_mate()
    phase("d_wait")
    arrived(st_recv.at[pl.ds(0, 7)], d_recv.at[1])
    arrived(o_recv.at[pl.ds(0, 7)], d_recv.at[0])
    phase("merge")
    whole_max = stats[qa, 0:1, :]
    for offset in range(1, 8):
        whole_max = jnp.maximum(whole_max, st_recv[ring(qa, offset), 0:1, :])
    weight = jnp.exp2(stats[qa, 0:1, :] - whole_max)
    whole_sum = stats[qa, 1:2, :] * weight
    whole_out = o_acc[qa, 0:128, :] * weight
    for offset in range(1, 8):
        slot = ring(qa, offset)
        weight = jnp.exp2(st_recv[slot, 0:1, :] - whole_max)
        whole_sum += st_recv[slot, 1:2, :] * weight
        whole_out += o_recv[slot].astype(F32) * weight
    lws_ref[...] = whole_max * (1.0 / LOG2E) + jnp.log(whole_sum)
    attended[...] = jnp.transpose(whole_out / whole_sum).astype(BF16)

    phase("heads")
    for far, xx, cc in ((1, 2, c), (1, 2, 1 - c), (0, 1, c), (0, 1, 1 - c), (0, 3, c), (0, 3, 1 - c), (0, 0, 1 - c)):
        peer = 2 * chip(xx) + cc
        rows = pl.ds(pl.multiple_of(peer * 32, 32), 32)
        push(attended.at[rows, :], heads.at[tp], AT, at_recv.at[far], (sp, peer))
    heads[tp] = attended[pl.ds(pl.multiple_of(tp * 32, 32), 32), :]
    phase("conv_sum")
    arrived(e_xrecv, ex_recv.at[0])
    e_own[3] = e_own[3] + e_xrecv[0].astype(F32) + e_xrecv[1].astype(F32) + e_xrecv[2].astype(F32)
    phase("w_wait")
    arrived(wa_all.at[pl.ds(0, 4)], w_recv.at[4])
    phase("heads_wait")
    arrived(heads.at[pl.ds(0, 5)], at_recv.at[0])
    phase("out")

    def heads_of(xx):
        slot = 2 * chip(xx)
        return jnp.concatenate([heads[slot], heads[slot + 1]], axis=1), slot

    near_heads = [heads_of(xx) for xx in (0, 1, 3)]
    for n in range(4):
        cols = slice(512 * n, 512 * n + 512)
        out = e_own[3, :, cols]
        for both, slot in near_heads:
            out += jnp.dot(both, wa_all[pl.ds(slot, 2), :, cols].reshape(256, 512), preferred_element_type=F32)
        e_own[3, :, cols] = out
    phase("far_wait")
    arrived(heads.at[pl.ds(0, 2)], at_recv.at[1])
    phase("far_out")
    both, slot = heads_of(2)
    for n in range(4):
        cols = slice(512 * n, 512 * n + 512)
        out = jnp.dot(both, wa_all[pl.ds(slot, 2), :, cols].reshape(256, 512), preferred_element_type=F32)
        mixed_ref[:, cols] = (out + e_own[3, :, cols]).astype(BF16)
    phase("send_wait")
    for ref, send in (
        (act_all.at[pl.ds(0, 7)], A),
        (lat_all.at[pl.ds(0, 7)], L),
        (q_all.at[pl.ds(0, 7)], Q),
        (kv_all.at[pl.ds(0, 7)], KV),
        (rope_all.at[pl.ds(0, 7)], R),
        (o_send.at[pl.ds(0, 7)], O),
        (stats.at[pl.ds(0, 7)], ST),
        (e_psend, EP),
        (e_xsend, EX),
        (halo_out, H),
        (wa_all.at[pl.ds(0, 7)], W),
        (heads.at[pl.ds(0, 7)], AT),
    ):
        remote(ref, ref, send, d_recv.at[0], mate).wait_send()
    phase(None)


def body(
    activations, norm_gain, query_weight, latent_weight, rope_key_weight, latent_gain, expand_weight,
    gate_weight, pre_weight, value_weight, conv_kernel, output_attend, output_conv,
):
    dma = pltpu.SemaphoreType.DMA
    vmem = pltpu.VMEM
    return pl.pallas_call(
        kernel,
        out_shape=(vmem((32, D), BF16), vmem((1, T), F32)),
        in_specs=[pl.BlockSpec(memory_space=pl.ANY)] * 14,
        out_specs=(pl.BlockSpec(memory_space=vmem), pl.BlockSpec(memory_space=vmem)),
        scratch_shapes=[
            vmem((8, T, 256), BF16),
            vmem((1, D), F32),
            vmem((1, 512), F32),
            vmem((512, 256), BF16),
            vmem((384, D), BF16),
            vmem((D, 384), BF16),
            vmem((3, 128), BF16),
            vmem((8, 128, D), BF16),
            vmem((128, D), BF16),
            vmem((320, 256), F32),
            vmem((T, 384), F32),
            vmem((T, 384), F32),
            vmem((8, 128, 128), BF16),
            vmem((8, Q_ROWS, 128), BF16),
            vmem((8, T, 256), BF16),
            vmem((8, KV_ROWS, 128), BF16),
            vmem((8, ROPE_ROWS, 128), BF16),
            vmem((8, T, 256), BF16),
            vmem((8, V_ROWS, T), BF16),
            vmem((8, 2 * T, T), F32),
            vmem((8, 2 * T, T), BF16),
            vmem((8, 8, T), F32),
            vmem((8, 8, T), F32),
            vmem((8, V_ROWS, T), F32),
            vmem((8, 128, T), BF16),
            vmem((8, 128, T), BF16),
            vmem((8, 8, T), F32),
            vmem((2, 8, 128), F32),
            vmem((2, 8, 128), F32),
            vmem((T, 128), BF16),
            vmem((T, 128), BF16),
            vmem((8, 32, 128), BF16),
            vmem((4, 32, D), BF16),
            vmem((4, 32, D), BF16),
            vmem((4, 32, D), F32),
            vmem((3, 32, D), BF16),
            vmem((3, 32, D), BF16),
            dma((10,)),
            dma((12,)),
            dma((11,)),
            dma((4,)),
            dma((5,)),
            dma((6,)),
            dma((5,)),
            dma((2,)),
            dma((1,)),
            dma((4,)),
            dma((1,)),
            dma((5,)),
            dma((2,)),
        ],
        compiler_params=pltpu.CompilerParams(collective_id=0, has_side_effects=True),
    )(
        activations, norm_gain.reshape(1, D), query_weight.T, latent_weight.T, rope_key_weight.T,
        latent_gain.reshape(1, 512), expand_weight, gate_weight, pre_weight, value_weight, conv_kernel,
        output_attend, output_conv, jnp.asarray(rotation_tables()),
    )


def solution(mesh):
    return jax.shard_map(
        body,
        mesh=mesh,
        in_specs=(
            P("sp", "tp"),
            P(),
            P(None, "tp"),
            P(None, "tp"),
            P(),
            P(),
            P(None, "tp"),
            P(None, "tp"),
            P(None, "tp"),
            P(None, "tp"),
            P(None, "tp"),
            P("tp", None),
            P("tp", None),
        ),
        out_specs=(P(("sp", "tp"), None), P("tp", "sp")),
        check_vma=False,
    )
```

```python
import functools

import jax
import jax.numpy as jnp
import numpy as np
from jax import lax
from jax.experimental import pallas as pl
from jax.experimental.pallas import tpu as pltpu
from jax.sharding import PartitionSpec as P

MESH = pl.DeviceIdType.MESH
F32 = jnp.float32
BF16 = jnp.bfloat16

D = 2048
NOPE = 128
ROPE = 64
GRID_W = 64
EPSILON = 1e-06
ROPE_BASE = 10000.0
RING = 8
NX = 4
T = 256
Q_ROWS = 384
KV_ROWS, ROPE_ROWS = 512, 128
V_ROWS = 144
LOW = -3.0e38
LOG2E = 1.4426950408889634


def rotation_tables():
    inverse = (np.float32(ROPE_BASE) ** (-np.arange(16, dtype=np.float32) / np.float32(16))).astype(np.float32)
    quarter = np.arange(128) // 16 % 4
    freq = inverse[np.arange(128) % 16]
    sign = np.where(quarter % 2 == 0, -1.0, 1.0)

    def table(count, mask):
        angle = (np.arange(count, dtype=np.float32)[:, None] * freq[None, :]).astype(np.float32)
        angle = angle.astype(np.float64)
        return np.concatenate([np.cos(angle) * mask, np.sin(angle) * sign * mask], axis=1).astype(np.float32)

    return np.concatenate([table(256, quarter < 2), table(GRID_W, quarter >= 2)])


def lane_iota(rows):
    return lax.broadcasted_iota(jnp.int32, (rows, 128), 1)


def kernel(
    act_hbm, gain_hbm, qw_hbm, lw_hbm, rw_hbm, lgain_hbm, ew_hbm, gw_hbm, pw_hbm, vw_hbm, ck_hbm, oa_hbm, oc_hbm,
    table_hbm,
    mixed_ref, lws_ref,
    act_all, gain, lgain, ew, wt, wb, ck, wa_all, wc, table, acc, acc_b, lat_all,
    q_all, q_cat, kv_all, rope_all, k_cat, vt_all, s_buf, w_buf, r_buf, stats, st_send, o_acc, o_send, o_recv, st_recv,
    halo_out, halo_in, conv_mixed, attended, heads, e_psend, e_precv, e_own, e_xsend, e_xrecv,
    load_sem, sent, a_recv, l_recv, q_recv, kv_recv, r_recv, d_recv, h_recv, ep_recv, ex_recv, w_recv, at_recv,
):
    sp = lax.axis_index("sp")
    tp = lax.axis_index("tp")
    x, c = lax.div(tp, 2), lax.rem(tp, 2)
    z, y = lax.div(sp, RING), lax.rem(sp, RING)
    ka, qa = y + c * (z - y), z + c * (y - z)
    k_stride, q_stride = 1 + 7 * c, 8 - 7 * c

    def ring(pos, offset):
        return lax.rem(pos + (offset + RING), RING)

    def k_dev(offset):
        return (sp + (ring(ka, offset) - ka) * k_stride, tp)

    def q_dev(offset):
        return (sp + (ring(qa, offset) - qa) * q_stride, tp)

    def chip(offset):
        return lax.rem(x + offset, NX)

    def t_dev(xx, cc):
        return (sp, 2 * xx + cc)

    scopes = []
    A, L, Q, KV, O, ST, EP, EX, H, W, AT, R = (sent.at[i] for i in range(12))

    def phase(name):
        if scopes:
            scopes.pop().__exit__(None, None, None)
        if name:
            scopes.append(jax.named_scope(name))
            scopes[-1].__enter__()

    def remote(src, dst, send, recv, dev):
        return pltpu.make_async_remote_copy(
            src_ref=src, dst_ref=dst, send_sem=send, recv_sem=recv, device_id=dev, device_id_type=MESH
        )

    def push(src, dst, send, recv, dev):
        remote(src, dst, send, recv, dev).start()

    def arrived(bytes_of, recv):
        remote(bytes_of, bytes_of, A, recv, t_dev(x, 1 - c)).wait_recv()

    phase("loads")
    def load(i, *pairs):
        for src, dst in pairs:
            pltpu.make_async_copy(src, dst, load_sem.at[i]).start()

    def loaded(i, ref):
        pltpu.make_async_copy(ref, ref, load_sem.at[i]).wait()

    load(0, (act_hbm, act_all.at[tp]))
    load(1, (gain_hbm, gain))
    load(
        2,
        (qw_hbm, wt.at[pl.ds(0, 192), :]),
        (rw_hbm, wt.at[pl.ds(192, 64), :]),
        (lw_hbm, wt.at[pl.ds(256, 64), :]),
        (lw_hbm, wt.at[pl.ds(320, 64), :]),
    )
    load(
        3,
        (gw_hbm, wb.at[:, pl.ds(0, 128)]),
        (pw_hbm, wb.at[:, pl.ds(128, 128)]),
        (vw_hbm, wb.at[:, pl.ds(256, 128)]),
    )
    load(4, (lgain_hbm, lgain))
    load(5, (table_hbm, table))
    load(6, (ck_hbm, ck))
    load(7, (ew_hbm, ew))
    load(8, (oa_hbm, wa_all.at[tp]))
    load(9, (oc_hbm, wc))

    phase("barrier")
    barrier = pltpu.get_barrier_semaphore()
    partners = [(sp, lax.rem(tp + k, 8)) for k in range(1, 8)]
    partners += [dev(k) for dev in (q_dev, k_dev) for k in (1, -1, 2, -2)]
    after, before = (lax.rem(sp + 1, 64), tp), (lax.rem(sp + 63, 64), tp)
    partners += [after, before]
    for dev in partners:
        pl.semaphore_signal(barrier, inc=1, device_id=dev, device_id_type=MESH)
    loaded(0, act_all.at[tp])
    pl.semaphore_wait(barrier, len(partners))

    phase("act_own")
    def rows_at(slot, ch, n):
        return act_all.at[slot, pl.ds(64 * ch, 64 * n), :]

    def a_push(slot, ch, n, recv, dev):
        push(rows_at(slot, ch, n), rows_at(slot, ch, n), A, a_recv.at[recv], dev)

    def a_wait(n, recv):
        arrived(act_all.at[0, pl.ds(0, 64 * n), :], a_recv.at[recv])

    up, down, mate = t_dev(chip(1), c), t_dev(chip(3), c), t_dev(x, 1 - c)
    for i in range(2):
        a_push(tp, i, 1, i, up)
        a_push(tp, 2 + i, 1, 3 + i, down)
    a_push(tp, 0, 4, 7, mate)
    a_push(tp, 2, 2, 2, up)
    a_push(tp, 0, 2, 5, down)
    loaded(1, gain)
    loaded(2, wt)
    loaded(3, wb)

    def project(slot, first):
        piece = act_all[slot].astype(F32)
        features = pl.ds(pl.multiple_of(slot * 256, 256), 256)
        scaled = (piece * gain[:, features]).astype(BF16)
        part = lax.dot_general(scaled, wt[:, features], (((1,), (1,)), ((), ())), preferred_element_type=F32)
        acc[...] = part if first else acc[...] + part
        part = jnp.dot(scaled, wb[features, :], preferred_element_type=F32)
        acc_b[...] = part if first else acc_b[...] + part
        squares = piece * piece
        return squares[:, 0:128] + squares[:, 128:256]

    squares = project(tp, True)
    phase("act_one")
    s_down, s_up, s_far = 2 * chip(3) + c, 2 * chip(1) + c, 2 * chip(2) + c
    other = 1 - 2 * c
    for i in range(2):
        a_wait(1, i)
        a_push(s_down, i, 1, 6, up)
        a_wait(1, 3 + i)
        a_push(s_up, 2 + i, 1, 6, down)
    a_wait(2, 2)
    a_push(s_down, 0, 4, 8, mate)
    a_wait(2, 5)
    a_push(s_up, 0, 4, 9, mate)
    a_wait(4, 7)
    squares += project(tp + other, False)
    squares += project(s_down, False)
    squares += project(s_up, False)
    a_wait(4, 8)
    squares += project(s_down + other, False)
    a_wait(4, 9)
    squares += project(s_up + other, False)
    phase("act_far")
    a_wait(4, 6)
    a_push(s_far, 0, 4, 10, mate)
    squares += project(s_far, False)
    a_wait(4, 10)
    squares += project(s_far + other, False)
    phase("latent_send")
    inv_rms = lax.rsqrt(jnp.sum(squares, axis=1, keepdims=True) / D + EPSILON)

    def w_push(slot, h, n, recv, dev):
        part = wa_all.at[slot, pl.ds(64 * h, 64 * n), :]
        push(part, part, W, w_recv.at[recv], dev)

    def w_start():
        w_push(tp, 0, 1, 0, up)
        w_push(tp, 1, 1, 1, down)
        w_push(tp, 0, 2, 4, mate)
        w_push(tp, 1, 1, 2, up)
        w_push(tp, 0, 1, 2, down)

    def w_onward():
        arrived(wa_all.at[0, pl.ds(0, 64), :], w_recv.at[0])
        w_push(s_down, 0, 1, 3, up)
        arrived(wa_all.at[0, pl.ds(0, 64), :], w_recv.at[1])
        w_push(s_up, 1, 1, 3, down)

    def w_near_to_mate():
        arrived(wa_all.at[0], w_recv.at[2])
        w_push(s_down, 0, 2, 4, mate)
        w_push(s_up, 0, 2, 4, mate)

    def w_far_to_mate():
        arrived(wa_all.at[0], w_recv.at[3])
        w_push(s_far, 0, 2, 4, mate)

    low = lane_iota(128) < 64
    latent_part = acc[:, 256:384] * inv_rms
    lat_all[tp] = jnp.where(low, latent_part[0:128], latent_part[128:256]).astype(BF16)

    def l_push(slot, recv, dev):
        push(lat_all.at[slot], lat_all.at[slot], L, l_recv.at[recv], dev)

    for i, dev in enumerate((t_dev(chip(2), c), up, down, mate)):
        l_push(tp, i, dev)
    loaded(8, wa_all.at[tp])
    w_start()

    phase("query")
    loaded(4, lgain)
    loaded(5, table)
    loaded(6, ck)
    loaded(7, ew)
    loaded(9, wc)
    scale = (NOPE + ROPE) ** (-0.5) * LOG2E
    q_all[qa, 0:256, :] = (acc[:, 0:128] * inv_rms * scale).astype(BF16)
    raw = acc[:, 128:256] * inv_rms
    even = lax.rem(lax.div(lane_iota(T), 16), 2) == 0
    tables = [table[pl.ds(sp * 4 + g, 1), :] + table[256:320, :] for g in range(4)]
    tables = jnp.concatenate(tables, axis=0)
    turned = jnp.where(even, pltpu.roll(raw, 112, 1), pltpu.roll(raw, 16, 1))
    rotated = raw * tables[:, 0:128] + turned * tables[:, 128:256]
    swapped = pltpu.roll(rotated, 64, 1)
    q_all[qa, 256:384, :] = (jnp.where(low, rotated[0:128], swapped[128:256]) * scale).astype(BF16)

    def spread(blocks, pos, rows, lead, stage, recv, dev):
        def move(offset, row, n, sem, to):
            part = blocks.at[ring(pos, offset), pl.ds(row, n), :]
            push(part, part, stage, recv.at[sem], dev(to))

        half, n = rows // 2, rows // 2 // lead

        def begin():
            for i in range(lead):
                move(0, i * n, n, i, 2)
                move(0, half + i * n, n, i, -2)
            move(0, 0, rows, lead + 1, 1)
            move(0, 0, rows, lead + 1, -1)
            move(0, half, half, lead, 2)
            move(0, 0, half, lead, -2)

        def onward_lead():
            for i in range(lead):
                arrived(blocks.at[0, pl.ds(0, 2 * n), :], recv.at[i])
                move(-2, i * n, n, lead + 3, 2)
                move(2, half + i * n, n, lead + 3, -2)
                move(-2, i * n, n, lead + 2, 1)
                move(2, half + i * n, n, lead + 2, -1)

        def onward_rest():
            arrived(blocks.at[0], recv.at[lead])
            move(-2, half, half, lead + 2, 1)
            move(2, 0, half, lead + 2, -1)

        def near():
            arrived(blocks.at[pl.ds(0, 2)], recv.at[lead + 1])

        def third():
            arrived(blocks.at[pl.ds(0, 2)], recv.at[lead + 2])

        def fourth():
            arrived(blocks.at[0], recv.at[lead + 3])

        return begin, onward_lead, onward_rest, near, third, fourth

    q_begin, q_onward_lead, q_onward_rest, q_near, q_third, q_fourth = spread(q_all, qa, Q_ROWS, 1, Q, q_recv, q_dev)
    r_begin, r_onward_lead, r_onward_rest, r_near, r_third, r_fourth = spread(rope_all, ka, ROPE_ROWS, 1, R, r_recv, k_dev)
    k_begin, k_onward_lead, k_onward_rest, k_near, k_third, k_fourth = spread(kv_all, ka, KV_ROWS, 2, KV, kv_recv, k_dev)
    q_begin()
    rope_all[ka] = jnp.where(low, swapped[0:128], rotated[128:256]).astype(BF16)

    def open_query(slot):
        paired = q_all[slot, 256:384, :].astype(F32)
        q_cat[slot, :, 0:128] = q_all[slot, 0:256, :]
        q_cat[slot, 0:128, 128:256] = jnp.where(low, paired, 0.0).astype(BF16)
        q_cat[slot, 128:256, 128:256] = jnp.where(low, pltpu.roll(paired, 64, 1), 0.0).astype(BF16)

    def open_keys(slot):
        paired = rope_all[slot]
        k_cat[slot, :, 0:128] = kv_all[slot, 0:256, :]
        k_cat[slot, 0:128, 128:256] = paired
        k_cat[slot, 128:256, 128:256] = pltpu.roll(paired.astype(F32), 64, 1).astype(BF16)
        vt_all[slot, 0:128, :] = jnp.transpose(kv_all[slot, 256:512, :].astype(F32)).astype(BF16)

    phase("halo")
    pre_mix = (acc_b[:, 128:256] * inv_rms) * (acc_b[:, 256:384] * inv_rms)
    pre_mix = pre_mix.astype(BF16).astype(F32)
    halo_out[0] = pre_mix[0:8]
    halo_out[1] = pre_mix[248:256]
    push(halo_out.at[0], halo_in.at[1], H, h_recv.at[0], before)
    push(halo_out.at[1], halo_in.at[0], H, h_recv.at[0], after)
    gate = acc_b[:, 0:128] * inv_rms

    phase("latent_wait")
    open_query(qa)
    stats[:, 0:1, :] = jnp.full((8, 1, T), LOW, F32)
    stats[:, 1:8, :] = jnp.zeros((8, 7, T), F32)
    o_acc[...] = jnp.zeros_like(o_acc)
    st_send[...] = jnp.zeros_like(st_send)
    ones = lax.broadcasted_iota(jnp.int32, (8, V_ROWS - 128, T), 1) == 0
    vt_all[:, 128:V_ROWS, :] = jnp.where(ones, 1.0, 0.0).astype(BF16)
    phase("latent_x")
    for recv, slot in ((1, s_down), (2, s_up), (0, s_far)):
        arrived(lat_all.at[0], l_recv.at[recv])
        l_push(slot, 3, mate)
    r_begin()
    phase("q2")
    q_onward_lead()
    phase("latent_mate")
    arrived(lat_all.at[pl.ds(0, 4)], l_recv.at[3])

    def pair(j):
        a, b = lat_all[2 * j].astype(F32), lat_all[2 * j + 1].astype(F32)
        return jnp.concatenate(
            [jnp.where(low, a, pltpu.roll(b, 64, 1)), jnp.where(low, pltpu.roll(a, 64, 1), b)], axis=0
        )

    phase("expand")
    parts = jnp.concatenate([pair(j) for j in range(4)], axis=1)
    latent_inv = lax.rsqrt(jnp.mean(parts * parts, axis=1, keepdims=True) + EPSILON)
    latent = (parts * latent_inv * lgain[...]).astype(BF16)
    expanded = jnp.dot(latent, ew[...], preferred_element_type=F32).astype(BF16)
    kv_all[ka, 0:256, :] = expanded[:, 0:128]
    kv_all[ka, 256:512, :] = expanded[:, 128:256]
    k_begin()
    phase("q2_rest")
    q_onward_rest()
    phase("conv")
    arrived(halo_in, h_recv.at[0])
    row = lax.broadcasted_iota(jnp.int32, (T, 128), 0)
    first = jnp.where(sp > 0, halo_in[0, 7:8, :], 0.0)
    last = jnp.where(sp < 63, halo_in[1, 0:1, :], 0.0)
    shifted_down = jnp.where(row == 0, first, pltpu.roll(pre_mix, 1, 0))
    shifted_up = jnp.where(row == T - 1, last, pltpu.roll(pre_mix, T - 1, 0))
    taps = ck[...].astype(F32)
    convolved = taps[0:1] * shifted_down + taps[1:2] * pre_mix + taps[2:3] * shifted_up
    conv_mixed[...] = (gate * convolved).astype(BF16)
    open_keys(ka)

    phase("conv_out")

    def rows_of(xx, cc):
        return pl.ds(pl.multiple_of((2 * xx + cc) * 32, 32), 32)

    order = [chip(2), chip(1), chip(3), x]
    for_mate = jnp.concatenate([conv_mixed[rows_of(xx, 1 - c), :] for xx in order], axis=0)
    for n in range(4):
        cols = slice(512 * n, 512 * n + 512)
        part = jnp.dot(for_mate, wc[:, cols], preferred_element_type=F32).astype(BF16)
        for j in range(4):
            e_psend[j, :, cols] = part[32 * j : 32 * j + 32]
    for j in range(4):
        push(e_psend.at[j], e_precv.at[j], EP, ep_recv.at[j], mate)
    for_own = jnp.concatenate([conv_mixed[rows_of(xx, c), :] for xx in order], axis=0)
    for n in range(4):
        cols = slice(512 * n, 512 * n + 512)
        part = jnp.dot(for_own, wc[:, cols], preferred_element_type=F32)
        for j in range(4):
            e_own[j, :, cols] = part[32 * j : 32 * j + 32]

    def key_blocks(ks, qs):
        n = len(ks) * T
        keys = jnp.concatenate([k_cat[k] for k in ks], axis=0)
        values = jnp.concatenate([vt_all[k] for k in ks], axis=1)
        for i, q in enumerate(qs):
            s_buf[i, 0:n] = lax.dot_general(keys, q_cat[q], (((1,), (1,)), ((), ())), preferred_element_type=F32)
        for i, q in enumerate(qs):
            scores = s_buf[i, 0:n]
            old_max = stats[q, 0:1, :]
            new_max = jnp.maximum(old_max, jnp.max(scores, axis=0, keepdims=True))
            r_buf[i, 0:1, :] = jnp.exp2(old_max - new_max)
            stats[q, 0:1, :] = new_max
            w_buf[i, 0:n] = jnp.exp2(scores - new_max).astype(BF16)
        for i, q in enumerate(qs):
            yield o_acc[q] * r_buf[i, 0:1, :] + jnp.dot(values, w_buf[i, 0:n], preferred_element_type=F32)

    def attend(ks, qs):
        for q, out in zip(qs, key_blocks(ks, qs)):
            o_acc[q] = out

    def d_push(offset):
        slot = ring(qa, offset)
        push(o_send.at[slot], o_recv.at[qa], O, d_recv.at[0], q_dev(offset))
        push(st_send.at[slot], st_recv.at[qa], ST, d_recv.at[1], q_dev(offset))

    def key_step(step, _):
        for s in (1, 2):

            @pl.when(step == s)
            def _(s=s):
                if s == 1:
                    r_near()
                    k_near()
                if s == 2:
                    k_onward_rest()
                for d in (s, -s):
                    open_keys(ring(ka, d))

        ks = (lax.rem(ka + step, RING), lax.rem(ka - step + RING, RING))
        attend(ks, range(8))
        return 0

    def conv_onward():
        for j in range(3):
            push(e_xsend.at[j], e_xrecv.at[j], EX, ex_recv.at[0], t_dev(order[j], c))

    phase("q_rest")
    q_near()
    for offset in (1, -1, 2, -2):
        open_query(ring(qa, offset))
    own = (ka,)
    phase("own_keys")
    attend(own, [ring(qa, offset) for offset in (0, 1, -1, 2, -2)])
    phase("rope_onward")
    r_onward_lead()
    r_onward_rest()
    phase("k_lead")
    k_onward_lead()
    phase("q3")
    q_third()
    for offset in (3, -3):
        open_query(ring(qa, offset))
    phase("q4")
    q_fourth()
    open_query(ring(qa, 4))

    phase("w_onward")
    w_onward()
    phase("own_rest")
    attend(own, [ring(qa, offset) for offset in (3, -3, 4)])
    phase("conv_mate")
    for j in range(4):
        arrived(e_precv.at[j], ep_recv.at[j])
        both = e_own[j] + e_precv[j].astype(F32)
        if j < 3:
            e_xsend[j] = both.astype(BF16)
        else:
            e_own[j] = both
    conv_onward()
    phase("keys")
    lax.fori_loop(1, 3, key_step, 0)
    phase("k4")
    r_fourth()
    k_fourth()
    open_keys(ring(ka, 4))
    attend((ring(ka, 4),), range(8))
    phase("k3")
    r_third()
    k_third()
    for d in (3, -3):
        open_keys(ring(ka, d))
    phase("last_keys")
    for offsets in ((4,), (3, 5), (2, 6), (1, 7, 0)):
        qs = [ring(qa, offset) for offset in offsets]
        for offset, q, out in zip(offsets, qs, key_blocks((ring(ka, 3), ring(ka, -3)), qs)):
            for half in range(2):
                lanes = slice(128 * half, 128 * half + 128)
                st_send[q, half : half + 1, :] = stats[q, 0:1, lanes]
                st_send[q, half + 2 : half + 3, :] = out[128:129, lanes]
            if offset:
                o_send[q] = out[0:128].astype(BF16)
            else:
                o_acc[qa] = out
        for offset in offsets:
            if offset:
                d_push(offset)
    phase("w_near")
    w_near_to_mate()
    phase("w_far")
    w_far_to_mate()
    phase("d_wait")
    arrived(st_recv.at[pl.ds(0, 7)], d_recv.at[1])
    arrived(o_recv.at[pl.ds(0, 7)], d_recv.at[0])
    phase("merge")
    def pair_of(ref, slot, i):
        return jnp.concatenate([ref[slot, i : i + 1, :], ref[slot, i + 1 : i + 2, :]], axis=1)

    slots = [ring(qa, offset) for offset in range(1, 8)]
    maxima = [pair_of(st_recv, slot, 0) for slot in slots]
    own_max = pair_of(st_send, qa, 0)
    whole_max = functools.reduce(jnp.maximum, maxima, own_max)
    weight = jnp.exp2(own_max - whole_max)
    whole_sum = pair_of(st_send, qa, 2) * weight
    whole_out = o_acc[qa, 0:128, :] * weight
    for slot, maximum in zip(slots, maxima):
        weight = jnp.exp2(maximum - whole_max)
        whole_sum += pair_of(st_recv, slot, 2) * weight
        whole_out += o_recv[slot].astype(F32) * weight
    lws_ref[...] = whole_max * (1.0 / LOG2E) + jnp.log(whole_sum)
    attended[...] = jnp.transpose(whole_out / whole_sum).astype(BF16)

    phase("heads")
    for far, xx, cc in ((1, 2, c), (1, 2, 1 - c), (0, 1, c), (0, 1, 1 - c), (0, 3, c), (0, 3, 1 - c), (0, 0, 1 - c)):
        peer = 2 * chip(xx) + cc
        rows = pl.ds(pl.multiple_of(peer * 32, 32), 32)
        push(attended.at[rows, :], heads.at[tp], AT, at_recv.at[far], (sp, peer))
    heads[tp] = attended[pl.ds(pl.multiple_of(tp * 32, 32), 32), :]
    phase("conv_sum")
    arrived(e_xrecv, ex_recv.at[0])
    e_own[3] = e_own[3] + e_xrecv[0].astype(F32) + e_xrecv[1].astype(F32) + e_xrecv[2].astype(F32)
    phase("w_wait")
    arrived(wa_all.at[pl.ds(0, 4)], w_recv.at[4])
    phase("heads_wait")
    arrived(heads.at[pl.ds(0, 5)], at_recv.at[0])
    phase("out")

    def heads_of(xx):
        slot = 2 * chip(xx)
        return jnp.concatenate([heads[slot], heads[slot + 1]], axis=1), slot

    near_heads = [heads_of(xx) for xx in (0, 1, 3)]
    for n in range(4):
        cols = slice(512 * n, 512 * n + 512)
        out = e_own[3, :, cols]
        for both, slot in near_heads:
            out += jnp.dot(both, wa_all[pl.ds(slot, 2), :, cols].reshape(256, 512), preferred_element_type=F32)
        e_own[3, :, cols] = out
    phase("far_wait")
    arrived(heads.at[pl.ds(0, 2)], at_recv.at[1])
    phase("far_out")
    both, slot = heads_of(2)
    for n in range(4):
        cols = slice(512 * n, 512 * n + 512)
        out = jnp.dot(both, wa_all[pl.ds(slot, 2), :, cols].reshape(256, 512), preferred_element_type=F32)
        mixed_ref[:, cols] = (out + e_own[3, :, cols]).astype(BF16)
    phase("send_wait")
    for ref, send in (
        (act_all.at[pl.ds(0, 7)], A),
        (lat_all.at[pl.ds(0, 7)], L),
        (q_all.at[pl.ds(0, 7)], Q),
        (kv_all.at[pl.ds(0, 7)], KV),
        (rope_all.at[pl.ds(0, 7)], R),
        (o_send.at[pl.ds(0, 7)], O),
        (st_send.at[pl.ds(0, 7)], ST),
        (e_psend, EP),
        (e_xsend, EX),
        (halo_out, H),
        (wa_all.at[pl.ds(0, 7)], W),
        (heads.at[pl.ds(0, 7)], AT),
    ):
        remote(ref, ref, send, d_recv.at[0], mate).wait_send()
    phase(None)


def body(
    activations, norm_gain, query_weight, latent_weight, rope_key_weight, latent_gain, expand_weight,
    gate_weight, pre_weight, value_weight, conv_kernel, output_attend, output_conv,
):
    dma = pltpu.SemaphoreType.DMA
    vmem = pltpu.VMEM
    return pl.pallas_call(
        kernel,
        out_shape=(vmem((32, D), BF16), vmem((1, T), F32)),
        in_specs=[pl.BlockSpec(memory_space=pl.ANY)] * 14,
        out_specs=(pl.BlockSpec(memory_space=vmem), pl.BlockSpec(memory_space=vmem)),
        scratch_shapes=[
            vmem((8, T, 256), BF16),
            vmem((1, D), F32),
            vmem((1, 512), F32),
            vmem((512, 256), BF16),
            vmem((384, D), BF16),
            vmem((D, 384), BF16),
            vmem((3, 128), BF16),
            vmem((8, 128, D), BF16),
            vmem((128, D), BF16),
            vmem((320, 256), F32),
            vmem((T, 384), F32),
            vmem((T, 384), F32),
            vmem((8, 128, 128), BF16),
            vmem((8, Q_ROWS, 128), BF16),
            vmem((8, T, 256), BF16),
            vmem((8, KV_ROWS, 128), BF16),
            vmem((8, ROPE_ROWS, 128), BF16),
            vmem((8, T, 256), BF16),
            vmem((8, V_ROWS, T), BF16),
            vmem((8, 2 * T, T), F32),
            vmem((8, 2 * T, T), BF16),
            vmem((8, 8, T), F32),
            vmem((8, 8, T), F32),
            vmem((8, 8, 128), F32),
            vmem((8, V_ROWS, T), F32),
            vmem((8, 128, T), BF16),
            vmem((8, 128, T), BF16),
            vmem((8, 8, 128), F32),
            vmem((2, 8, 128), F32),
            vmem((2, 8, 128), F32),
            vmem((T, 128), BF16),
            vmem((T, 128), BF16),
            vmem((8, 32, 128), BF16),
            vmem((4, 32, D), BF16),
            vmem((4, 32, D), BF16),
            vmem((4, 32, D), F32),
            vmem((3, 32, D), BF16),
            vmem((3, 32, D), BF16),
            dma((10,)),
            dma((12,)),
            dma((11,)),
            dma((4,)),
            dma((5,)),
            dma((6,)),
            dma((5,)),
            dma((2,)),
            dma((1,)),
            dma((4,)),
            dma((1,)),
            dma((5,)),
            dma((2,)),
        ],
        compiler_params=pltpu.CompilerParams(collective_id=0, has_side_effects=True),
    )(
        activations, norm_gain.reshape(1, D), query_weight.T, latent_weight.T, rope_key_weight.T,
        latent_gain.reshape(1, 512), expand_weight, gate_weight, pre_weight, value_weight, conv_kernel,
        output_attend, output_conv, jnp.asarray(rotation_tables()),
    )


def solution(mesh):
    return jax.shard_map(
        body,
        mesh=mesh,
        in_specs=(
            P("sp", "tp"),
            P(),
            P(None, "tp"),
            P(None, "tp"),
            P(),
            P(),
            P(None, "tp"),
            P(None, "tp"),
            P(None, "tp"),
            P(None, "tp"),
            P(None, "tp"),
            P("tp", None),
            P("tp", None),
        ),
        out_specs=(P(("sp", "tp"), None), P("tp", "sp")),
        check_vma=False,
    )
```
